256 devices in a mesh: sp: 64 (over z, x, core), tp: 4 (over y).
Axes of the slice: x: 4, y: 4, z: 8, core: 2. Of those that a mesh axis runs over, the one named last changes fastest.
Arguments:
- queries: bfloat16 [40960, 2048], P('sp', 'tp'), may hold values from -164 to 164
- keys: bfloat16 [40960, 512], P('sp', 'tp'), may hold values from -6 to 6
- values: bfloat16 [40960, 512], P('sp', 'tp'), may hold values from -6 to 6
- sink: float32 [32], P('tp'), may hold values from 4 to 8
- stream: bfloat16 [40960, 2048], P(('sp', 'tp')), may hold values from -6 to 6
- out_weight: bfloat16 [2048, 2048], P('tp'), may hold values from -0.5390625 to 0.5390625
- norm_gain: float32 [2048], replicated, may hold values from 0.1 to 1.9
- gate_weight: bfloat16 [2048, 5632], P('sp', 'tp'), may hold values from -0.125 to 0.125
- up_weight: bfloat16 [2048, 5632], P('sp', 'tp'), may hold values from -0.125 to 0.125
- down_weight: bfloat16 [5632, 2048], P('tp', 'sp'), may hold values from -0.23925781 to 0.23925781
Outputs:
- result: bfloat16 [40960, 2048], P(('sp', 'tp'))
The draws below stay inside these ranges and needn't reach their ends.
All inputs are finite; a program needn't handle non-finite values.
Results may differ from the reference program's by a relative error of at most 0.019.
Values may be sent and summed in bfloat16 or wider, within the bound.
A program may use at most 128 MiB of HBM per device.

```python
import jax
import jax.numpy as jnp
from jax import lax

D = 2048
HEADS = 32
KV_HEADS = 8
HEAD = 64
FF = 5632
WINDOW = 128
TOK_DEV = 640
TOKENS = 40960


def draw_queries(key, part):
    shape = (TOKENS, HEADS * HEAD)
    return jnp.clip(2.0 * jax.random.normal(key, shape, jnp.float32), -12.0, 12.0).astype(jnp.bfloat16)


def block_scale(key, shape, cuts, least, largest):
    def one(axis_at, shards_of):
        steps = jax.random.uniform(jax.random.fold_in(jax.random.fold_in(key, 6), axis_at), (shards_of,), jnp.float32, least / len(cuts), largest / len(cuts))
        return jnp.repeat(jnp.exp(steps), shape[axis_at] // shards_of).reshape((-1,) + (1,) * (len(shape) - axis_at - 1))

    gain = one(*cuts[0])
    for cut in cuts[1:]:
        gain = gain * one(*cut)
    return gain


def normal_values(own_key, extent, width, bound, cuts=(), held_as=jnp.bfloat16):
    level = block_scale(own_key, extent, cuts, -0.22, 0.18) if cuts else 1.0
    array = jax.random.normal(own_key, extent, jnp.float32) * width * level
    return jnp.minimum(jnp.maximum(array, -bound), bound).astype(held_as)


def setup_inputs(seed: int = 0) -> dict:
    key_list = jax.random.split(jax.random.key(seed), 11)
    return {
        "queries": draw_queries(jax.random.fold_in(key_list[10], 71), 0),
        "keys": normal_values(key_list[1], (TOKENS, KV_HEADS * HEAD), 1.0, 6.0, ((0, 64), (1, 4))),
        "values": normal_values(key_list[2], (TOKENS, KV_HEADS * HEAD), 1.0, 6.0, ((0, 64), (1, 4))),
        "sink": jnp.clip(4.0 + 4.0 * jax.random.uniform(key_list[3], (HEADS,), jnp.float32) ** block_scale(key_list[3], (HEADS,), ((0, 4),), -0.2, 0.2), 4.0, 8.0),
        "stream": normal_values(key_list[4], (TOKENS, D), 1.0, 6.0, ((0, 256),)),
        "out_weight": normal_values(key_list[5], (HEADS * HEAD, D), 0.09, 0.5390625, ((0, 4),)),
        "norm_gain": jnp.clip(1.0 + 0.18 * jax.random.normal(key_list[6], (D,), jnp.float32), 0.1, 1.9),
        "gate_weight": normal_values(key_list[7], (D, FF), D ** -0.5, 0.125, ((0, 64), (1, 4))),
        "up_weight": normal_values(key_list[8], (D, FF), D ** -0.5, 0.125, ((0, 64), (1, 4))),
        "down_weight": normal_values(key_list[9], (FF, D), 0.04, 0.23925781, ((0, 4), (1, 64))),
    }


def rotary(block, start):
    length = block.shape[0]
    middle = HEAD // 2
    inverse = 1.0 / 10000.0 ** (jnp.arange(0, HEAD, 2, dtype=jnp.float32) / HEAD)
    places = (start + jnp.arange(length, dtype=jnp.int32)).astype(jnp.float32)
    angles = places[:, None, None] * inverse[None, None, :]
    cosine_table = jnp.cos(angles)
    sine_table = jnp.sin(angles)
    pieces = block.astype(jnp.float32).reshape(length, -1, HEAD)
    leading = pieces[..., :middle]
    trailing = pieces[..., middle:]
    turned = jnp.concatenate([leading * cosine_table - trailing * sine_table, trailing * cosine_table + leading * sine_table], -1)
    return turned.reshape(length, -1).astype(jnp.bfloat16)

def reference(queries, keys, values, sink, stream, out_weight, norm_gain, gate_weight, up_weight, down_weight):
    length = queries.shape[0]
    blocks = length // WINDOW
    group = HEADS // KV_HEADS
    kv_width = KV_HEADS * HEAD
    turned_q = rotary(queries, 0)
    turned_k = rotary(keys, 0)
    paired = jnp.concatenate([turned_k, values], 1)
    padded = jnp.pad(paired, ((WINDOW, WINDOW), (0, 0)))
    framed = padded.reshape(blocks + 2, WINDOW, 2 * kv_width)
    banded = jnp.concatenate([framed[:-2], framed[1:-1], framed[2:]], axis=1)
    key_band = jnp.moveaxis(banded[..., :kv_width].reshape(blocks, 3 * WINDOW, KV_HEADS, HEAD), 2, 0)
    value_band = jnp.moveaxis(banded[..., kv_width:].reshape(blocks, 3 * WINDOW, KV_HEADS, HEAD), 2, 0)
    query_blocks = jnp.moveaxis(turned_q.reshape(blocks, WINDOW, KV_HEADS, group, HEAD), 2, 0)
    sink_grid = sink.reshape(KV_HEADS, group)
    query_place = jnp.arange(blocks)[:, None, None] * WINDOW + jnp.arange(WINDOW)[None, :, None]
    key_place = jnp.arange(blocks)[:, None, None] * WINDOW - WINDOW + jnp.arange(3 * WINDOW)[None, None, :]
    valid = (jnp.abs(key_place - query_place) <= WINDOW) & (key_place >= 0) & (key_place < length)

    def one_head(item):
        query_part, key_part, value_part, sink_part = item
        scores = jnp.einsum('nqgd,nsd->ngqs', query_part.astype(jnp.float32), key_part.astype(jnp.float32)) * HEAD ** (-0.5)
        scores = jnp.where(valid[:, None], scores, -jnp.inf)
        sink_here = sink_part[None, :, None]
        top = jnp.maximum(lax.optimization_barrier(jnp.max(scores, -1)), sink_here)
        raised = jnp.exp(scores - top[..., None])
        denom = lax.optimization_barrier(jnp.sum(raised, -1)) + jnp.exp(sink_here - top)
        weights = lax.optimization_barrier((raised / denom[..., None]).astype(jnp.bfloat16))
        output = jnp.einsum('ngqs,nsd->nqgd', weights.astype(jnp.float32), value_part.astype(jnp.float32))
        return output.astype(jnp.bfloat16)
    heads_out = lax.map(one_head, (query_blocks, key_band, value_band, sink_grid))
    attended = jnp.moveaxis(heads_out, 0, 2).reshape(length, HEADS * HEAD)
    mixed = (stream.astype(jnp.float32) + jnp.dot(attended, out_weight, preferred_element_type=jnp.float32)).astype(jnp.bfloat16)
    mixed_wide = mixed.astype(jnp.float32)
    scale = lax.rsqrt(lax.optimization_barrier(jnp.mean(mixed_wide * mixed_wide, -1, keepdims=True)) + 1e-06)
    normed = (mixed_wide * scale * norm_gain).astype(jnp.bfloat16)

    def feed_forward(rows):
        gate = jnp.dot(rows, gate_weight, preferred_element_type=jnp.float32)
        upward = jnp.dot(rows, up_weight, preferred_element_type=jnp.float32)
        hidden = (jax.nn.silu(gate) * upward).astype(jnp.bfloat16)
        return jnp.dot(hidden, down_weight, preferred_element_type=jnp.float32)
    lowered = lax.map(feed_forward, normed.reshape(-1, TOK_DEV, D)).reshape(length, D)
    return (mixed_wide + 0.5 * lowered).astype(jnp.bfloat16)
```

```python
import jax
import jax.numpy as jnp
import numpy as np
from jax import lax
from jax.experimental import pallas as pl
from jax.experimental.pallas import tpu as pltpu
from jax.sharding import PartitionSpec as P

HEAD = 64
WINDOW = 128
MESH = pl.DeviceIdType.MESH
BF = jnp.bfloat16
F32 = jnp.float32

NZ, NX, NC, NY = 8, 4, 2, 4
ROWS = 32
TOK = 640
BLK = TOK // NY
HALF = BLK // 2
EXT = TOK + 2 * WINDOW
PAD = 3 * BLK + 4 * WINDOW
D = 2048
FFL = 1408
GB = 1280
CB = 2 * GB
CA = 2 * (FFL - GB) + FFL
QW = 512
NSEM = 112


def tables():
    lane = (np.arange(128) % 64) % 32
    freq = 1.0 / 10000.0 ** (2.0 * lane / HEAD)
    near = (np.arange(EXT) - WINDOW)[:, None] * freq[None]
    far = (np.arange(NZ * NX * NC) * TOK)[:, None] * freq[None]
    return np.concatenate([np.cos(near), np.sin(near), np.cos(far), np.sin(far)], 0).astype(np.float32)


def nt(a, b):
    return lax.dot_general(a, b, (((1,), (1,)), ((), ())), preferred_element_type=F32)


def mm(a, b):
    return jnp.dot(a, b, preferred_element_type=F32)


def kernel(
    q_hbm, k_hbm, v_hbm, sink, st_hbm, ow_hbm, gain, g_hbm, u_hbm, d_hbm, tab_hbm,
    out,
    wa, wb, tab, q, qr, kv, kk, vv, ow, dn, st, bias, att,
    pb1, s1, f1, pb2, s2, f2, mixed, xs, hid,
    lsem, ssem, rsem,
):
    s = lax.axis_index("sp")
    y = lax.axis_index("tp")
    c = s % NC
    x = (s // NC) % NX
    z = s // (NC * NX)

    def at(zz, xx, cc):
        return ((zz % NZ) * NX + xx % NX) * NC + cc

    ydev = {1: (s, (y + 1) % NY), -1: (s, (y + NY - 1) % NY)}
    xdev = {1: (at(z, x + 1, c), y), -1: (at(z, x + NX - 1, c), y)}
    zdev = {1: (at(z + 1, x, c), y), -1: (at(z + NZ - 1, x, c), y)}
    mate = (at(z, x, 1 - c), y)
    nsp = NZ * NX * NC
    hdev = {1: ((s + 1) % nsp, y), -1: ((s + nsp - 1) % nsp, y)}

    loads = {}

    def load(name, src, dst):
        cp = pltpu.make_async_copy(src, dst, lsem.at[len(loads)])
        cp.start()
        loads[name] = cp

    rest = FFL - GB
    load("gb", g_hbm.at[:, pl.ds(0, GB)], wb.at[z, x, c, :, pl.ds(0, GB)])
    load("ub", u_hbm.at[:, pl.ds(0, GB)], wb.at[z, x, c, :, pl.ds(GB, GB)])
    load("d", d_hbm, dn)
    load("ga", g_hbm.at[:, pl.ds(GB, rest)], wa.at[z, x, c, :, pl.ds(0, rest)])
    load("ua", u_hbm.at[:, pl.ds(GB, rest)], wa.at[z, x, c, :, pl.ds(rest, rest)])
    load("k", k_hbm, kv.at[0, pl.ds(WINDOW, TOK)])
    load("v", v_hbm, kv.at[1, pl.ds(WINDOW, TOK)])
    load("tab", tab_hbm, tab)
    load("q", q_hbm, q)
    load("ow", ow_hbm, ow)
    load("st", st_hbm, st)

    barrier = pltpu.get_barrier_semaphore()
    for dev in (*ydev.values(), *xdev.values(), *zdev.values(), mate, *hdev.values()):
        pl.semaphore_signal(barrier, inc=1, device_id=dev, device_id_type=MESH)
    pl.semaphore_wait(barrier, 9)

    slots = {}
    sent = []

    def copy(name, src, dst, dev):
        i = slots.setdefault(name, len(slots))
        return pltpu.make_async_remote_copy(
            src_ref=src, dst_ref=dst, send_sem=ssem.at[i], recv_sem=rsem.at[i], device_id=dev, device_id_type=MESH
        )

    def send(name, ref, dev, dst=None):
        cp = copy(name, ref, ref if dst is None else dst, dev)
        cp.start()
        sent.append(cp)

    def recv(name, ref):
        copy(name, ref, ref, mate).wait_recv()

    def zb(dz, half=None):
        ref = wb.at[(z + dz + NZ) % NZ, x, c]
        return ref if half is None else ref.at[pl.ds(16 * half, 16)]

    def xb(dz, dx, half=None):
        ref = wb.at[(z + dz + NZ) % NZ, (x + dx + NX) % NX, c]
        return ref if half is None else ref.at[pl.ds(16 * half, 16)]

    def za(dz, half=None):
        zz = (z + dz + NZ) % NZ
        return wa.at[zz, :, c] if half is None else wa.at[zz, pl.ds(2 * half, 2), c]

    def xa(dx, half=None):
        ref = wa.at[z, (x + dx + NX) % NX, c]
        return ref if half is None else ref.at[pl.ds(16 * half, 16)]

    def bx_send(dz):
        for r in (1, -1):
            send(("bx", dz, r), xb(dz, 0), xdev[r])

    def bx_mid(dz):
        for r, half in ((1, 0), (-1, 1)):
            recv(("bx", dz, r), xb(dz, -r))
            send(("bh", dz, r), xb(dz, -r, half), xdev[r])

    def bx_end(dz):
        for r, half in ((1, 0), (-1, 1)):
            recv(("bh", dz, r), xb(dz, -2 * r, half))
        zz = (z + dz + NZ) % NZ
        send(("bm", dz), wb.at[zz, :, c], mate)

    def bz(n):
        for r, half in ((1, 0), (-1, 1)):
            if n < 4:
                recv(("bz", r, n), zb(-r * n))
                if n < 3:
                    send(("bz", r, n + 1), zb(-r * n), zdev[r])
                else:
                    send(("bz", r, 4), zb(-r * 3, half), zdev[r])
            else:
                recv(("bz", r, 4), zb(-r * 4, half))
        if n < 4:
            bx_send(n)
            bx_send(-n)
        else:
            bx_send(4)

    def az(n):
        for r, half in ((1, 0), (-1, 1)):
            if n < 4:
                recv(("az", r, n), za(-r * n))
                if n < 3:
                    send(("az", r, n + 1), za(-r * n), zdev[r])
                else:
                    send(("az", r, 4), za(-r * 3, half), zdev[r])
            else:
                recv(("az", r, 4), za(-r * 4, half))
        for dz in (n, -n) if n < 4 else (4,):
            send(("am", dz), za(dz), mate)

    def ax_mid():
        for r, half in ((1, 0), (-1, 1)):
            recv(("ax", r), xa(-r))
            send(("ah", r), xa(-r, half), xdev[r])

    def ax_end():
        for r, half in ((1, 0), (-1, 1)):
            recv(("ah", r), xa(-2 * r, half))
        for r in (1, -1):
            send(("az", r, 1), za(0), zdev[r])
        send(("am", 0), za(0), mate)

    def mates():
        for dz in (0, 1, -1, 2, -2, 3, -3, 4):
            zz = (z + dz + NZ) % NZ
            recv(("bm", dz), wb.at[zz, :, 1 - c])
            recv(("am", dz), wa.at[zz, :, 1 - c])

    loads["gb"].wait()
    loads["ub"].wait()
    for r in (1, -1):
        send(("bz", r, 1), zb(0), zdev[r])
    loads["k"].wait()
    loads["v"].wait()
    send(("halo", -1), kv.at[:, pl.ds(WINDOW, WINDOW)], hdev[-1], kv.at[:, pl.ds(WINDOW + TOK, WINDOW)])
    send(("halo", 1), kv.at[:, pl.ds(TOK, WINDOW)], hdev[1], kv.at[:, pl.ds(0, WINDOW)])
    loads["d"].wait()
    eye = (
        lax.broadcasted_iota(jnp.int32, (ROWS, ROWS), 0) == lax.broadcasted_iota(jnp.int32, (ROWS, ROWS), 1)
    ).astype(F32).astype(BF)
    wa[z, x, c, :, 2 * rest :] = nt(eye, dn[...]).astype(BF)
    loads["ga"].wait()
    loads["ua"].wait()
    for r in (1, -1):
        send(("ax", r), xa(0), xdev[r])
    bx_send(0)

    loads["tab"].wait()
    cb = tab[pl.ds(2 * EXT + s, 1), :]
    sb = tab[pl.ds(2 * EXT + nsp + s, 1), :]

    def rotate(rows, value):
        cl, sl = tab[rows, :], tab[pl.ds(EXT + rows.start, rows.size), :]
        cos = cb * cl - sb * sl
        sin = sb * cl + cb * sl
        return value.astype(F32) * cos + mm(value, turn) * sin

    jj = lax.broadcasted_iota(jnp.int32, (128, 128), 0)
    ii = lax.broadcasted_iota(jnp.int32, (128, 128), 1)
    low = (ii % 64) < 32
    turn = (jnp.where(jj == ii - 32, jnp.where(low, 0.0, 1.0), 0.0)
            - jnp.where(jj == ii + 32, jnp.where(low, 1.0, 0.0), 0.0)).astype(BF)
    flip = jnp.where((jj + 64) % 128 == ii, 1.0, 0.0).astype(BF)

    loads["q"].wait()
    for t in range(4):
        qr[t] = rotate(pl.ds(WINDOW, TOK), q[:, 128 * t : 128 * (t + 1)]).astype(BF)
    ax_mid()
    recv(("halo", -1), kv.at[:, pl.ds(WINDOW + TOK, WINDOW)])
    recv(("halo", 1), kv.at[:, pl.ds(0, WINDOW)])
    lane = lax.broadcasted_iota(jnp.int32, (EXT, 128), 1)
    left = lane < 64
    zero = jnp.zeros((EXT, 128), BF)
    one = jnp.where(left, 1.0, 0.0).astype(BF)
    two = jnp.where(left, 0.0, 1.0).astype(BF)
    kr = rotate(pl.ds(0, EXT), kv[0]).astype(BF)
    ks = mm(kr, flip)
    kr = kr.astype(F32)
    vr = kv[1].astype(F32)
    vs = mm(kv[1], flip)
    for i in range(4):
        kk[i, EXT:, :] = jnp.zeros((PAD - EXT, 128), BF)
        vv[i, EXT:, :] = jnp.zeros((PAD - EXT, 256), BF)
        ksrc, vsrc = ((kr, vr), (ks, vs), (ks, vs), (kr, vr))[i]
        keep = left if i % 2 == 0 else lane >= 64
        kk[i, :EXT, :] = jnp.where(keep, ksrc, 0.0).astype(BF)
        vv[i, :EXT, :128] = jnp.where(keep, vsrc, 0.0).astype(BF)
        vv[i, :EXT, 128:] = one if i % 2 == 0 else two

    def attend(b):
        first = s * TOK + b * BLK
        ri = lax.broadcasted_iota(jnp.int32, (BLK, QW), 0)
        ci = lax.broadcasted_iota(jnp.int32, (BLK, QW), 1)
        lo = jnp.maximum(ri, WINDOW - first)
        hi = jnp.minimum(ri + 2 * WINDOW, nsp * TOK - 1 + WINDOW - first)
        bias[...] = jnp.where((ci >= lo) & (ci <= hi), 0.0, -jnp.inf)
        rows = pl.multiple_of(b * BLK, 32)
        half = lax.broadcasted_iota(jnp.int32, (BLK, 128), 1) < 64

        def tile(t, carry):
            qt = qr[t, pl.ds(rows, BLK), :]
            acc, ends = None, []
            for par in range(2):
                i = (t // 2) * 2 + par
                sc = nt(qt, kk[i, pl.ds(rows, QW), :]) * 0.125 + bias[...]
                snk = sink[2 * t + par]
                top = jnp.maximum(jnp.max(sc, axis=1, keepdims=True), snk)
                prob = jnp.exp(sc - top).astype(BF)
                part = mm(prob, vv[i, pl.ds(rows, QW), :])
                acc = part if acc is None else acc + part
                ends.append(jnp.exp(snk - top))
            den = acc[:, 128:] + jnp.where(half, ends[0], ends[1])
            att[:, pl.ds(pl.multiple_of(t * 128, 128), 128)] = (acc[:, :128] / den).astype(BF)
            return carry

        lax.fori_loop(0, 4, tile, 0)

    def project(slot):
        def cols(n, carry):
            at_n = pl.ds(pl.multiple_of(n * 512, 512), 512)
            pb1[slot, :, at_n] = mm(att[...], ow[:, at_n]).astype(BF)
            return carry

        lax.fori_loop(0, 4, cols, 0)

    UP, LOW = pl.ds(0, HALF), pl.ds(HALF, HALF)
    part_of = {1: (0, UP, LOW), -1: (1, LOW, UP)}

    def rs_far(tag, pb, sbuf):
        for r in (1, -1):
            j, rel, _ = part_of[r]
            send((tag, "s", r), pb.at[0, rel], ydev[r], sbuf.at[j])

    def rs_near(tag, pb, fbuf, r):
        j, _, direct = part_of[r]
        send((tag, "d", r), pb.at[1 + j, direct], ydev[r], fbuf.at[j, direct])

    def rs_relay(tag, pb, sbuf, fbuf):
        for r in (1, -1):
            j, rel, _ = part_of[r]
            recv((tag, "s", r), sbuf.at[j])
            pb[1 + j, rel, :] = (pb[1 + j, rel, :].astype(F32) + sbuf[j].astype(F32)).astype(BF)
            send((tag, "r", r), pb.at[1 + j, rel], ydev[r], fbuf.at[j, rel])

    def rs_sum(tag, pb, fbuf):
        for r in (1, -1):
            j, rel, direct = part_of[r]
            recv((tag, "d", r), fbuf.at[j, direct])
            recv((tag, "r", r), fbuf.at[j, rel])
        return pb[3].astype(F32) + fbuf[0].astype(F32) + fbuf[1].astype(F32)

    ynext = {2: (y + 2) % NY, 1: (y + 1) % NY, -1: (y + NY - 1) % NY, 0: y}

    bx_mid(0)
    attend(ynext[2])
    loads["ow"].wait()
    project(0)
    rs_far("r1", pb1, s1)
    bz(1)
    ax_end()
    attend(ynext[1])
    project(1)
    rs_near("r1", pb1, f1, 1)
    bx_end(0)
    attend(ynext[-1])
    project(2)
    rs_near("r1", pb1, f1, -1)
    bz(2)
    attend(y)
    project(3)
    bx_mid(1)
    bx_mid(-1)
    rs_relay("r1", pb1, s1, f1)
    az(1)
    bz(3)
    bx_end(1)
    bx_end(-1)
    bx_mid(2)
    bx_mid(-2)
    loads["st"].wait()
    total = st[...].astype(F32) + rs_sum("r1", pb1, f1)
    mixed[...] = total.astype(BF)
    wide = mixed[...].astype(F32)
    scale = lax.rsqrt(jnp.mean(wide * wide, axis=1, keepdims=True) + 1e-06)
    xs[y] = (wide * scale * gain[...]).astype(BF)
    for r in (1, -1):
        for part in part_of[r][1:]:
            send(("g", r, part is UP), xs.at[y, part], ydev[r])
    az(2)
    bz(4)
    bx_end(2)
    bx_end(-2)
    for r in (1, -1):
        rel = part_of[r][1]
        recv(("g", r, rel is UP), xs.at[ynext[-r], rel])
        send(("gh", r), xs.at[ynext[-r], rel], ydev[r])
    bx_mid(3)
    bx_mid(-3)
    az(3)
    bx_end(3)
    bx_end(-3)
    bx_mid(4)
    for r in (1, -1):
        direct = part_of[r][2]
        recv(("g", r, direct is UP), xs.at[ynext[-r], direct])
    az(4)
    bx_end(4)
    mates()

    def feed(b, slot):
        def cols(n, carry):
            gu = []
            for base in (0, GB):
                w = wb[:, :, :, :, pl.ds(pl.multiple_of(base + n * 256, 256), 256)].reshape(D, 256)
                gu.append(mm(xs[b], w))
            hid[:, pl.ds(pl.multiple_of(n * 256, 256), 256)] = (gu[0] / (1.0 + jnp.exp(-gu[0])) * gu[1]).astype(BF)
            return carry

        lax.fori_loop(0, GB // 256, cols, 0)
        gu = mm(xs[b], wa[:, :, :, :, : 2 * rest].reshape(D, 2 * rest))
        gate, upward = gu[:, :rest], gu[:, rest:]
        hid[:, GB:] = (gate / (1.0 + jnp.exp(-gate)) * upward).astype(BF)

        def down(n, carry):
            w = wa[n, :, :, :, 2 * rest :].reshape(256, FFL)
            pb2[slot, :, pl.ds(pl.multiple_of(n * 256, 256), 256)] = nt(hid[...], w).astype(BF)
            return carry

        lax.fori_loop(0, D // 256, down, 0)

    feed(ynext[1], 1)
    rs_near("r2", pb2, f2, 1)
    feed(ynext[-1], 2)
    rs_near("r2", pb2, f2, -1)
    for r in (1, -1):
        rel = part_of[r][1]
        recv(("gh", r), xs.at[ynext[2], rel])
    feed(ynext[2], 0)
    rs_far("r2", pb2, s2)
    feed(y, 3)
    rs_relay("r2", pb2, s2, f2)
    out[...] = (mixed[...].astype(F32) + 0.5 * rs_sum("r2", pb2, f2)).astype(BF)
    for cp in sent:
        cp.wait_send()
    assert len(slots) <= NSEM


def local(queries, keys, values, sink, stream, out_weight, norm_gain, gate_weight, up_weight, down_weight):
    hbm = pl.BlockSpec(memory_space=pl.ANY)
    vmem = pl.BlockSpec(memory_space=pltpu.VMEM)
    smem = pl.BlockSpec(memory_space=pltpu.SMEM)
    V = pltpu.VMEM
    return pl.pallas_call(
        kernel,
        name="layer",
        out_shape=jax.ShapeDtypeStruct((BLK, D), BF),
        in_specs=[hbm, hbm, hbm, smem, hbm, hbm, vmem, hbm, hbm, hbm, hbm],
        out_specs=vmem,
        scratch_shapes=[
            V((NZ, NX, NC, ROWS, CA), BF),
            V((NZ, NX, NC, ROWS, CB), BF),
            V((2 * EXT + 2 * NZ * NX * NC, 128), F32),
            V((TOK, 512), BF),
            V((4, TOK, 128), BF),
            V((2, EXT, 128), BF),
            V((4, PAD, 128), BF),
            V((4, PAD, 256), BF),
            V((512, D), BF),
            V((FFL, ROWS), BF),
            V((BLK, D), BF),
            V((BLK, QW), F32),
            V((BLK, 512), BF),
            V((4, BLK, D), BF),
            V((2, HALF, D), BF),
            V((2, BLK, D), BF),
            V((4, BLK, D), BF),
            V((2, HALF, D), BF),
            V((2, BLK, D), BF),
            V((BLK, D), BF),
            V((NY, BLK, D), BF),
            V((BLK, FFL), BF),
            pltpu.SemaphoreType.DMA((11,)),
            pltpu.SemaphoreType.DMA((NSEM,)),
            pltpu.SemaphoreType.DMA((NSEM,)),
        ],
        compiler_params=pltpu.CompilerParams(
            collective_id=0, has_side_effects=True, vmem_limit_bytes=62 * 1024 * 1024
        ),
    )(
        queries, keys, values, sink, stream, out_weight, norm_gain.reshape(1, D),
        gate_weight, up_weight, down_weight, jnp.asarray(tables()),
    )


def solution(mesh):
    placed = (
        P("sp", "tp"), P("sp", "tp"), P("sp", "tp"), P("tp"), P(("sp", "tp"), None), P("tp", None), P(),
        P("sp", "tp"), P("sp", "tp"), P("tp", "sp"),
    )
    return jax.shard_map(local, mesh=mesh, in_specs=placed, out_specs=P(("sp", "tp"), None), check_vma=False)
```

```python
import jax
import jax.numpy as jnp
import numpy as np
from jax import lax
from jax.experimental import pallas as pl
from jax.experimental.pallas import tpu as pltpu
from jax.sharding import PartitionSpec as P

HEAD = 64
WINDOW = 128
MESH = pl.DeviceIdType.MESH
BF = jnp.bfloat16
F32 = jnp.float32

NZ, NX, NC, NY = 8, 4, 2, 4
ROWS = 32
TOK = 640
BLK = TOK // NY
HALF = BLK // 2
EXT = TOK + 2 * WINDOW
PAD = 3 * BLK + 4 * WINDOW
D = 2048
FFL = 1408
GB = 1280
CB = 2 * GB
CA = 2 * (FFL - GB) + FFL
QW = 512
NSEM = 192
ORDER = (
    "begin", "turn_q", "prepare", "att_f", "bz_1", "proj_f", "ax_mid", "att_n", "proj_n", "az_1_0", "bm_0", "att_p",
    "rl+0", "bz_2", "proj_p", "rl-0", "bm_1", "att_o", "rl+1", "near+", "rl-1", "proj_o", "ax_end", "az_1_-1",
    "az_2_0", "be_0", "az_1_1", "bm_-1", "bm_2", "bz_3", "norm_U", "az_1_2", "bm_-2", "az_2_-1", "be_1", "be_-1",
    "az_3_0", "be_2", "norm_L", "az_2_1", "bz_4", "bm_3", "az_2_2", "bm_-3", "az_3_-1", "gU", "az_4_0", "be_-2",
    "az_3_1", "gL0", "bm_4", "az_3_2", "az_4_-1", "be_3", "gL1", "az_4_1", "be_-3", "az_4_2", "be_4", "feed1",
    "feed2", "feed3", "r2l0", "r2l1", "fin0", "fin1",
)
SUB = 2


def tables():
    lane = (np.arange(128) % 64) % 32
    freq = 1.0 / 10000.0 ** (2.0 * lane / HEAD)
    near = (np.arange(EXT) - WINDOW)[:, None] * freq[None]
    far = (np.arange(NZ * NX * NC) * TOK)[:, None] * freq[None]
    return np.concatenate([np.cos(near), np.sin(near), np.cos(far), np.sin(far)], 0).astype(np.float32)


def nt(a, b):
    return lax.dot_general(a, b, (((1,), (1,)), ((), ())), preferred_element_type=F32)


def mm(a, b):
    return jnp.dot(a, b, preferred_element_type=F32)


def kernel(
    q_hbm, k_hbm, v_hbm, sink, st_hbm, ow_hbm, gain, g_hbm, u_hbm, d_hbm, tab_hbm,
    out,
    wa, wb, tab, q, qr, kv, kk, vv, ow, st, bias, att,
    pb1, s1, f1, pb2, s2, f2, mixed, xs, hid,
    lsem, ssem, rsem,
):
    s = lax.axis_index("sp")
    y = lax.axis_index("tp")
    c = s % NC
    x = (s // NC) % NX
    z = s // (NC * NX)

    def at(zz, xx, cc):
        return ((zz % NZ) * NX + xx % NX) * NC + cc

    ydev = {1: (s, (y + 1) % NY), -1: (s, (y + NY - 1) % NY)}
    xdev = {1: (at(z, x + 1, c), y), -1: (at(z, x + NX - 1, c), y)}
    zdev = {1: (at(z + 1, x, c), y), -1: (at(z + NZ - 1, x, c), y)}
    mate = (at(z, x, 1 - c), y)
    nsp = NZ * NX * NC
    hdev = {1: ((s + 1) % nsp, y), -1: ((s + nsp - 1) % nsp, y)}

    barrier = pltpu.get_barrier_semaphore()
    for dev in (*ydev.values(), *xdev.values(), *zdev.values(), mate, *hdev.values()):
        pl.semaphore_signal(barrier, inc=1, device_id=dev, device_id_type=MESH)

    loads = {}

    def load(name, src, dst):
        cp = pltpu.make_async_copy(src, dst, lsem.at[len(loads)])
        cp.start()
        loads[name] = cp

    rest = FFL - GB
    load("k", k_hbm, kv.at[0, pl.ds(WINDOW, TOK)])
    load("v", v_hbm, kv.at[1, pl.ds(WINDOW, TOK)])
    load("gb", g_hbm.at[:, pl.ds(0, GB)], wb.at[z, x, c, :, pl.ds(0, GB)])
    load("ub", u_hbm.at[:, pl.ds(0, GB)], wb.at[z, x, c, :, pl.ds(GB, GB)])
    load("da", d_hbm, wa.at[z, x, c, :, pl.ds(2 * rest, FFL)])
    load("ga", g_hbm.at[:, pl.ds(GB, rest)], wa.at[z, x, c, :, pl.ds(0, rest)])
    load("ua", u_hbm.at[:, pl.ds(GB, rest)], wa.at[z, x, c, :, pl.ds(rest, rest)])
    load("tab", tab_hbm, tab)
    load("q", q_hbm, q)
    load("ow", ow_hbm, ow)
    load("st", st_hbm, st)

    def greet():
        pl.semaphore_wait(barrier, 9)

    greet()

    slots = {}
    sent = []

    def copy(name, src, dst, dev):
        i = slots.setdefault(name, len(slots))
        return pltpu.make_async_remote_copy(
            src_ref=src, dst_ref=dst, send_sem=ssem.at[i], recv_sem=rsem.at[i], device_id=dev, device_id_type=MESH
        )

    def send(name, ref, dev, dst=None):
        cp = copy(name, ref, ref if dst is None else dst, dev)
        cp.start()
        sent.append(cp)

    def recv(name, ref):
        copy(name, ref, ref, mate).wait_recv()

    def zb(dz, half=None):
        ref = wb.at[(z + dz + NZ) % NZ, x, c]
        return ref if half is None else ref.at[pl.ds(16 * half, 16)]

    def xb(dz, dx, half=None):
        ref = wb.at[(z + dz + NZ) % NZ, (x + dx + NX) % NX, c]
        return ref if half is None else ref.at[pl.ds(16 * half, 16)]

    def za(dz, dx, half=None):
        ref = wa.at[(z + dz + NZ) % NZ, (x + dx + NX) % NX, c]
        return ref if half is None else ref.at[pl.ds(16 * half, 16)]

    def xa(dx, half=None):
        ref = wa.at[z, (x + dx + NX) % NX, c]
        return ref if half is None else ref.at[pl.ds(16 * half, 16)]

    def bx_send(dz):
        for r in (1, -1):
            send(("bx", dz, r), xb(dz, 0), xdev[r])

    def bx_mid(dz):
        for r, half in ((1, 0), (-1, 1)):
            recv(("bx", dz, r), xb(dz, -r))
            send(("bh", dz, r), xb(dz, -r, half), xdev[r])

    def bx_end(dz):
        for r, half in ((1, 0), (-1, 1)):
            recv(("bh", dz, r), xb(dz, -2 * r, half))
        zz = (z + dz + NZ) % NZ
        send(("bm", dz), wb.at[zz, :, c], mate)

    def bz(n):
        for r, half in ((1, 0), (-1, 1)):
            if n < 4:
                recv(("bz", r, n), zb(-r * n))
                if n < 3:
                    send(("bz", r, n + 1), zb(-r * n), zdev[r])
                else:
                    send(("bz", r, 4), zb(-r * 3, half), zdev[r])
            else:
                recv(("bz", r, 4), zb(-r * 4, half))
        if n < 4:
            bx_send(n)
            bx_send(-n)
        else:
            bx_send(4)

    def az_send(n, dx, r):
        if n < 4:
            send(("az", r, n, dx), za(-r * (n - 1), dx), zdev[r])
        else:
            half = 0 if r == 1 else 1
            send(("az", r, 4, dx), za(-r * 3, dx, half), zdev[r])

    parts = {}

    def az(n, *dxs):
        for dx in dxs:
            for r, half in ((1, 0), (-1, 1)):
                if n < 4:
                    recv(("az", r, n, dx), za(-r * n, dx))
                    az_send(n + 1, dx, r)
                else:
                    recv(("az", r, 4, dx), za(-r * 4, dx, half))
            parts[n] = parts.get(n, 0) + 1
            if parts[n] == NX:
                for dz in (n, -n) if n < 4 else (4,):
                    send(("am", dz), wa.at[(z + dz + NZ) % NZ, :, c], mate)

    def ax_mid():
        for r, half in ((1, 0), (-1, 1)):
            recv(("ax", r), xa(-r))
            send(("ah", r), xa(-r, half), xdev[r])
        for r in (1, -1):
            for dx in (1, -1):
                az_send(1, dx, r)

    def ax_end():
        for r, half in ((1, 0), (-1, 1)):
            recv(("ah", r), xa(-2 * r, half))
        for r in (1, -1):
            az_send(1, 2, r)
        send(("am", 0), wa.at[z, :, c], mate)

    def mates():
        for dz in (0, 1, -1, 2, -2, 3, -3, 4):
            zz = (z + dz + NZ) % NZ
            recv(("bm", dz), wb.at[zz, :, 1 - c])
            recv(("am", dz), wa.at[zz, :, 1 - c])

    def begin():
        loads["k"].wait()
        loads["v"].wait()
        send(("halo", -1), kv.at[:, pl.ds(WINDOW, WINDOW)], hdev[-1], kv.at[:, pl.ds(WINDOW + TOK, WINDOW)])
        send(("halo", 1), kv.at[:, pl.ds(TOK, WINDOW)], hdev[1], kv.at[:, pl.ds(0, WINDOW)])
        for name in ("gb", "ub", "ga", "ua", "da"):
            loads[name].wait()
        for r in (1, -1):
            send(("bz", r, 1), zb(0), zdev[r])
            send(("ax", r), xa(0), xdev[r])
        for r in (1, -1):
            az_send(1, 0, r)
        bx_send(0)

    loads["tab"].wait()
    cb = tab[pl.ds(2 * EXT + s, 1), :]
    sb = tab[pl.ds(2 * EXT + nsp + s, 1), :]

    def rotate(rows, value):
        cl, sl = tab[rows, :], tab[pl.ds(EXT + rows.start, rows.size), :]
        cos = cb * cl - sb * sl
        sin = sb * cl + cb * sl
        return value.astype(F32) * cos + mm(value, turn) * sin

    jj = lax.broadcasted_iota(jnp.int32, (128, 128), 0)
    ii = lax.broadcasted_iota(jnp.int32, (128, 128), 1)
    low = (ii % 64) < 32
    turn = (jnp.where(jj == ii - 32, jnp.where(low, 0.0, 1.0), 0.0)
            - jnp.where(jj == ii + 32, jnp.where(low, 1.0, 0.0), 0.0)).astype(BF)
    flip = jnp.where((jj + 64) % 128 == ii, 1.0, 0.0).astype(BF)

    def turn_q():
        loads["q"].wait()
        for t in range(4):
            qr[t] = rotate(pl.ds(WINDOW, TOK), q[:, 128 * t : 128 * (t + 1)]).astype(BF)

    def prepare():
        recv(("halo", -1), kv.at[:, pl.ds(WINDOW + TOK, WINDOW)])
        recv(("halo", 1), kv.at[:, pl.ds(0, WINDOW)])
        lane = lax.broadcasted_iota(jnp.int32, (EXT, 128), 1)
        left = lane < 64
        one = jnp.where(left, 1.0, 0.0).astype(BF)
        two = jnp.where(left, 0.0, 1.0).astype(BF)
        kr = rotate(pl.ds(0, EXT), kv[0]).astype(BF)
        ks = mm(kr, flip)
        kr = kr.astype(F32)
        vr = kv[1].astype(F32)
        vs = mm(kv[1], flip)
        for i in range(4):
            kk[i, EXT:, :] = jnp.zeros((PAD - EXT, 128), BF)
            vv[i, EXT:, :] = jnp.zeros((PAD - EXT, 256), BF)
            ksrc, vsrc = ((kr, vr), (ks, vs), (ks, vs), (kr, vr))[i]
            keep = left if i % 2 == 0 else lane >= 64
            kk[i, :EXT, :] = jnp.where(keep, ksrc, 0.0).astype(BF)
            vv[i, :EXT, :128] = jnp.where(keep, vsrc, 0.0).astype(BF)
            vv[i, :EXT, 128:] = one if i % 2 == 0 else two

    def attend(b):
        first = s * TOK + b * BLK
        ri = lax.broadcasted_iota(jnp.int32, (BLK, QW), 0)
        ci = lax.broadcasted_iota(jnp.int32, (BLK, QW), 1)
        lo = jnp.maximum(ri, WINDOW - first)
        hi = jnp.minimum(ri + 2 * WINDOW, nsp * TOK - 1 + WINDOW - first)
        bias[...] = jnp.where((ci >= lo) & (ci <= hi), 0.0, -jnp.inf)
        rows = pl.multiple_of(b * BLK, 32)
        half = lax.broadcasted_iota(jnp.int32, (BLK, 128), 1) < 64

        def tile(t, carry):
            qt = qr[t, pl.ds(rows, BLK), :]
            acc, ends = None, []
            for par in range(2):
                i = (t // 2) * 2 + par
                sc = nt(qt, kk[i, pl.ds(rows, QW), :]) * 0.125 + bias[...]
                snk = sink[2 * t + par]
                top = jnp.maximum(jnp.max(sc, axis=1, keepdims=True), snk)
                prob = jnp.exp(sc - top).astype(BF)
                part = mm(prob, vv[i, pl.ds(rows, QW), :])
                acc = part if acc is None else acc + part
                ends.append(jnp.exp(snk - top))
            den = acc[:, 128:] + jnp.where(half, ends[0], ends[1])
            att[:, pl.ds(pl.multiple_of(t * 128, 128), 128)] = (acc[:, :128] / den).astype(BF)
            return carry

        lax.fori_loop(0, 4, tile, 0)

    UP, LOW = 0, 1
    at_half = {("n", LOW): 0, ("p", UP): 1, ("f", UP): 2, ("f", LOW): 3, ("n", UP): 4, ("p", LOW): 5, ("o", UP): 6, ("o", LOW): 7}
    ahead = {1: "n", -1: "p"}
    back = {1: "p", -1: "n"}
    via = {1: UP, -1: LOW}
    cols_of = [pl.ds(i * (D // SUB), D // SUB) for i in range(SUB)]

    def project(block):
        def cols(n, carry):
            at_n = pl.ds(pl.multiple_of(n * 512, 512), 512)
            done = mm(att[...], ow[:, at_n]).astype(BF)
            for part in (UP, LOW):
                pb1[at_half[block, part], :, at_n] = done[part * HALF : (part + 1) * HALF]
            return carry

        lax.fori_loop(0, 4, cols, 0)

    def rs_far(tag, pb, sbuf):
        for i, cols in enumerate(cols_of):
            for r in (1, -1):
                send((tag, "s", r, i), pb.at[at_half["f", via[r]], :, cols], ydev[r], sbuf.at[via[r], :, cols])

    def rs_near(tag, pb, fbuf, r):
        part = 1 - via[r]
        send((tag, "d", r), pb.at[at_half[ahead[r], part]], ydev[r], fbuf.at[part, via[r]])

    def rs_relay(tag, pb, sbuf, fbuf, r, i):
        cols, part = cols_of[i], via[r]
        j = at_half[ahead[r], part]
        recv((tag, "s", r, i), sbuf.at[part, :, cols])
        pb[j, :, cols] = (pb[j, :, cols].astype(F32) + sbuf[part, :, cols].astype(F32)).astype(BF)
        send((tag, "r", r, i), pb.at[j, :, cols], ydev[r], fbuf.at[part, via[r], :, cols])

    def rs_sum(tag, pb, fbuf, part, i=None):
        r = 1 if part == UP else -1
        if not i:
            recv((tag, "d", -r), fbuf.at[part, via[-r]])
        for k, cols in enumerate(cols_of):
            if i is None or i == k:
                recv((tag, "r", r, k), fbuf.at[part, via[r], :, cols])
        cols = slice(None) if i is None else cols_of[i]
        own = pb[at_half["o", part], :, cols].astype(F32)
        return own + fbuf[part, 0, :, cols].astype(F32) + fbuf[part, 1, :, cols].astype(F32)

    ynext = {"f": (y + 2) % NY, "n": (y + 1) % NY, "p": (y + NY - 1) % NY, "o": y}

    def normalise(part):
        rows = pl.ds(part * HALF, HALF)
        total = st[rows, :].astype(F32) + rs_sum("r1", pb1, f1, part)
        mixed[rows, :] = total.astype(BF)
        wide = mixed[rows, :].astype(F32)
        scale = lax.rsqrt(jnp.mean(wide * wide, axis=1, keepdims=True) + 1e-06)
        xs[at_half["o", part]] = (wide * scale * gain[...]).astype(BF)

    def g_cols(part):
        return cols_of if part == LOW else [pl.ds(0, D)]

    def g_send(part):
        for i, cols in enumerate(g_cols(part)):
            for r in (1, -1):
                send(("g", r, part, i), xs.at[at_half["o", part], :, cols], ydev[r], xs.at[at_half[back[r], part], :, cols])

    def g_recv(part, i):
        cols = g_cols(part)[i]
        for r in (1, -1):
            ref = xs.at[at_half[back[r], part], :, cols]
            recv(("g", r, part, i), ref)
            if via[r] == part:
                send(("gh", r, i), ref, ydev[r], xs.at[at_half["f", part], :, cols])

    def g_far():
        for r in (1, -1):
            for i, cols in enumerate(g_cols(via[r])):
                recv(("gh", r, i), xs.at[at_half["f", via[r]], :, cols])

    def feed(first, count):
        many = count * HALF
        rows = pl.ds(0, many)

        def cols(n, carry):
            gu = []
            for base in (0, GB):
                w = wb[:, :, :, :, pl.ds(pl.multiple_of(base + n * 256, 256), 256)].reshape(D, 256)
                gu.append(mm(xs[first : first + count].reshape(many, D), w))
            hid[rows, pl.ds(pl.multiple_of(n * 256, 256), 256)] = (gu[0] / (1.0 + jnp.exp(-gu[0])) * gu[1]).astype(BF)
            return carry

        lax.fori_loop(0, GB // 256, cols, 0, unroll=True)
        gu = mm(xs[first : first + count].reshape(many, D), wa[:, :, :, :, : 2 * rest].reshape(D, 2 * rest))
        gate, upward = gu[:, :rest], gu[:, rest:]
        hid[rows, GB:] = (gate / (1.0 + jnp.exp(-gate)) * upward).astype(BF)

        def down(n, carry):
            w = wa[pl.ds(2 * n, 2), :, :, :, 2 * rest :].reshape(512, FFL)
            at_n = pl.ds(pl.multiple_of(n * 512, 512), 512)
            pb2[first : first + count, :, at_n] = nt(hid[rows, :], w).astype(BF).reshape(count, HALF, 512)
            return carry

        lax.fori_loop(0, D // 512, down, 0)

    def near2():
        rs_near("r2", pb2, f2, 1)
        rs_near("r2", pb2, f2, -1)

    def relay2(i):
        for r in (1, -1):
            rs_relay("r2", pb2, s2, f2, r, i)

    def attend_on(block):
        if block == "o":
            loads["st"].wait()
        attend(ynext[block])

    def project_on(block):
        if block == "f":
            loads["ow"].wait()
        project(block)
        if block == "f":
            rs_far("r1", pb1, s1)
        if block == "p":
            rs_near("r1", pb1, f1, -1)

    def norm_on(part):
        normalise(part)
        g_send(part)

    steps = {
        "begin": begin,
        "turn_q": turn_q,
        "prepare": prepare,
        "near+": lambda: rs_near("r1", pb1, f1, 1),
        "norm_U": lambda: norm_on(UP),
        "norm_L": lambda: norm_on(LOW),
        "gU": lambda: g_recv(UP, 0),
        "gL0": lambda: g_recv(LOW, 0),
        "gL1": lambda: g_recv(LOW, 1),
        "ax_mid": ax_mid,
        "ax_end": ax_end,
        "feed1": lambda: (mates(), feed(0, 2), near2()),
        "feed2": lambda: (g_far(), feed(2, 2), rs_far("r2", pb2, s2)),
        "feed3": lambda: feed(4, 4),
        "r2l0": lambda: relay2(0),
        "r2l1": lambda: relay2(1),
        "fin0": lambda: finish(0),
        "fin1": lambda: finish(1),
    }

    def run_steps(name):
        if name in steps:
            return steps[name]()
        head, *rest_of = name.split("_")
        if head == "att":
            return attend_on(rest_of[0])
        if head == "proj":
            return project_on(rest_of[0])
        if head[:2] == "rl":
            return rs_relay("r1", pb1, s1, f1, 1 if head[2] == "+" else -1, int(head[3]))
        numbers = [int(n) for n in rest_of]
        return {"bz": bz, "bm": bx_mid, "be": bx_end, "az": az}[head](*numbers)

    def finish(i):
        cols = cols_of[i]
        for part in (UP, LOW):
            rows = pl.ds(part * HALF, HALF)
            out[rows, cols] = mixed[rows, cols].astype(F32) + 0.5 * rs_sum("r2", pb2, f2, part, i)

    for name in ORDER:
        run_steps(name)

    def drain():
        for cp in sent:
            cp.wait_send()

    drain()
    assert len(slots) <= NSEM


def local(queries, keys, values, sink, stream, out_weight, norm_gain, gate_weight, up_weight, down_weight):
    hbm = pl.BlockSpec(memory_space=pl.ANY)
    vmem = pl.BlockSpec(memory_space=pltpu.VMEM)
    smem = pl.BlockSpec(memory_space=pltpu.SMEM)
    V = pltpu.VMEM
    done = pl.pallas_call(
        kernel,
        name="layer",
        out_shape=jax.ShapeDtypeStruct((BLK, D), F32),
        in_specs=[hbm, hbm, hbm, smem, hbm, hbm, vmem, hbm, hbm, hbm, hbm],
        out_specs=vmem,
        scratch_shapes=[
            V((NZ, NX, NC, ROWS, CA), BF),
            V((NZ, NX, NC, ROWS, CB), BF),
            V((2 * EXT + 2 * NZ * NX * NC, 128), F32),
            V((TOK, 512), BF),
            V((4, TOK, 128), BF),
            V((2, EXT, 128), BF),
            V((4, PAD, 128), BF),
            V((4, PAD, 256), BF),
            V((512, D), BF),
            V((BLK, D), BF),
            V((BLK, QW), F32),
            V((BLK, 512), BF),
            V((8, HALF, D), BF),
            V((2, HALF, D), BF),
            V((2, 2, HALF, D), BF),
            V((8, HALF, D), BF),
            V((2, HALF, D), BF),
            V((2, 2, HALF, D), BF),
            V((BLK, D), BF),
            V((8, HALF, D), BF),
            V((2 * BLK, FFL), BF),
            pltpu.SemaphoreType.DMA((11,)),
            pltpu.SemaphoreType.DMA((NSEM,)),
            pltpu.SemaphoreType.DMA((NSEM,)),
        ],
        compiler_params=pltpu.CompilerParams(
            collective_id=0, has_side_effects=True, vmem_limit_bytes=62 * 1024 * 1024
        ),
    )(
        queries, keys, values, sink, stream, out_weight, norm_gain.reshape(1, D),
        gate_weight, up_weight, down_weight.T, jnp.asarray(tables()),
    )
    return done.astype(BF)


def solution(mesh):
    placed = (
        P("sp", "tp"), P("sp", "tp"), P("sp", "tp"), P("tp"), P(("sp", "tp"), None), P("tp", None), P(),
        P("sp", "tp"), P("sp", "tp"), P("tp", "sp"),
    )
    return jax.shard_map(local, mesh=mesh, in_specs=placed, out_specs=P(("sp", "tp"), None), check_vma=False)
```

```python
import jax
import jax.numpy as jnp
import numpy as np
from jax import lax
from jax.experimental import pallas as pl
from jax.experimental.pallas import tpu as pltpu
from jax.sharding import PartitionSpec as P

HEAD = 64
WINDOW = 128
MESH = pl.DeviceIdType.MESH
BF = jnp.bfloat16
F32 = jnp.float32

NZ, NX, NC, NY = 8, 4, 2, 4
ROWS = 32
TOK = 640
BLK = TOK // NY
HALF = BLK // 2
EXT = TOK + 2 * WINDOW
PAD = 3 * BLK + 4 * WINDOW
D = 2048
FFL = 1408
GB = 1280
CB = 2 * GB
CA = 2 * (FFL - GB) + FFL
QW = 512
NRECV = 62
NSEND = 14
ORDER = (
    "begin", "turn_q", "prep_own", "prepare", "att_f", "bz_1", "proj_f", "ax_mid", "bm_0", "az_1_0", "att_n",
    "proj_n", "att_p", "rl+0", "bz_2", "proj_p", "rl-0", "att_o", "rl+1", "near+", "rl-1", "proj_o", "ax_end",
    "bm_1", "az_1_1", "bm_-1", "az_1_-1", "az_2_0", "be_0", "tr_0", "bm_2", "bz_3", "norm_U", "az_1_2", "bm_-2",
    "tr_1", "tr_-1", "az_2_1", "be_1", "be_-1", "az_2_-1", "be_2", "norm_L", "az_3_0", "bz_4", "bm_3", "az_2_2",
    "tr_2", "tr_-2", "bm_-3", "az_3_1", "gU", "be_-2", "az_3_-1", "az_4_0", "gL0", "bm_4", "az_3_2", "az_4_1",
    "be_3", "tr_3", "tr_-3", "gL1", "az_4_-1", "be_-3", "az_4_2", "be_4", "tr_4", "feed1", "near0", "near1", "feed2",
    "feed3", "r2l0", "r2l1", "fin0", "fin1",
)
SUB = 2


def tables():
    lane = (np.arange(128) % 64) % 32
    freq = 1.0 / 10000.0 ** (2.0 * lane / HEAD)
    near = (np.arange(EXT) - WINDOW)[:, None] * freq[None]
    far = (np.arange(NZ * NX * NC) * TOK)[:, None] * freq[None]
    return np.concatenate([np.cos(near), np.sin(near), np.cos(far), np.sin(far)], 0).astype(np.float32)


def nt(a, b):
    return lax.dot_general(a, b, (((1,), (1,)), ((), ())), preferred_element_type=F32)


def mm(a, b):
    return jnp.dot(a, b, preferred_element_type=F32)


def kernel(
    q_hbm, k_hbm, v_hbm, sink, st_hbm, ow_hbm, gain, g_hbm, u_hbm, d_hbm, tab_hbm,
    out,
    wa, wb, tab, q, qr, kv, kk, vv, ow, st, bias, att,
    pb1, s1, f1, pb2, s2, f2, mixed, xs, hid, dt,
    lsem, ssem, rsem,
):
    s = lax.axis_index("sp")
    y = lax.axis_index("tp")
    c = s % NC
    x = (s // NC) % NX
    z = s // (NC * NX)

    def at(zz, xx, cc):
        return ((zz % NZ) * NX + xx % NX) * NC + cc

    ydev = {1: (s, (y + 1) % NY), -1: (s, (y + NY - 1) % NY)}
    xdev = {1: (at(z, x + 1, c), y), -1: (at(z, x + NX - 1, c), y)}
    zdev = {1: (at(z + 1, x, c), y), -1: (at(z + NZ - 1, x, c), y)}
    mate = (at(z, x, 1 - c), y)
    nsp = NZ * NX * NC
    hdev = {1: ((s + 1) % nsp, y), -1: ((s + nsp - 1) % nsp, y)}

    barrier = pltpu.get_barrier_semaphore()
    for dev in (*ydev.values(), *xdev.values(), *zdev.values(), mate, *hdev.values()):
        pl.semaphore_signal(barrier, inc=1, device_id=dev, device_id_type=MESH)

    loads = {}

    def load(name, src, dst):
        i = loads.setdefault(name, len(loads))
        pltpu.make_async_copy(src, dst, lsem.at[i]).start()

    def loaded(name, ref):
        pltpu.make_async_copy(ref, ref, lsem.at[loads[name]]).wait()

    rest = FFL - GB
    load("kv", k_hbm, kv.at[0, pl.ds(WINDOW, TOK)])
    load("kv", v_hbm, kv.at[1, pl.ds(WINDOW, TOK)])
    load("b", g_hbm.at[:, pl.ds(0, GB)], wb.at[z, x, c, :, pl.ds(0, GB)])
    load("b", u_hbm.at[:, pl.ds(0, GB)], wb.at[z, x, c, :, pl.ds(GB, GB)])
    load("a", d_hbm, wa.at[z, x, c, :, pl.ds(2 * rest, FFL)])
    load("a", g_hbm.at[:, pl.ds(GB, rest)], wa.at[z, x, c, :, pl.ds(0, rest)])
    load("a", u_hbm.at[:, pl.ds(GB, rest)], wa.at[z, x, c, :, pl.ds(rest, rest)])
    load("tab", tab_hbm, tab)
    load("q", q_hbm, q)
    load("ow", ow_hbm, ow)
    load("st", st_hbm, st)

    def greet():
        pl.semaphore_wait(barrier, 9)

    greet()

    taken, given = {}, {}

    def send(key, kind, ref, dev, dst=None):
        i = taken.setdefault(key, len(taken))
        k = given.setdefault(kind, len(given))
        pltpu.make_async_remote_copy(
            src_ref=ref, dst_ref=ref if dst is None else dst, send_sem=ssem.at[k], recv_sem=rsem.at[i],
            device_id=dev, device_id_type=MESH,
        ).start()

    def recv(key, ref):
        i = taken.setdefault(key, len(taken))
        pltpu.make_async_copy(ref, ref, rsem.at[i]).wait()

    def zb(dz, half=None):
        ref = wb.at[(z + dz + NZ) % NZ, x, c]
        return ref if half is None else ref.at[pl.ds(16 * half, 16)]

    def xb(dz, dx, half=None):
        ref = wb.at[(z + dz + NZ) % NZ, (x + dx + NX) % NX, c]
        return ref if half is None else ref.at[pl.ds(16 * half, 16)]

    def za(dz, dx, half=None):
        ref = wa.at[(z + dz + NZ) % NZ, (x + dx + NX) % NX, c]
        return ref if half is None else ref.at[pl.ds(16 * half, 16)]

    def xa(dx, half=None):
        ref = wa.at[z, (x + dx + NX) % NX, c]
        return ref if half is None else ref.at[pl.ds(16 * half, 16)]

    oneb, onea = wb.at[0, 0, 0], wa.at[0, 0, 0]
    twob, twoa = wb.at[pl.ds(0, 2), 0, 0], wa.at[pl.ds(0, 2), 0, 0]
    way = ((1, 0), (-1, 1))

    def b_mate(dz, dx):
        send(("bm",), "bm", xb(dz, dx), mate)

    def a_mate(dz, dx):
        send(("am", dz), "am", za(dz, dx), mate)

    def bx_send(dz):
        for r in (1, -1):
            send(("bx", dz), "bx", xb(dz, 0), xdev[r])
        b_mate(dz, 0)

    def bx_mid(dz):
        recv(("bx", dz), twob)
        for r, half in way:
            send(("bh", dz), "bh", xb(dz, -r, half), xdev[r])
        for r in (1, -1):
            b_mate(dz, r)

    def bx_end(dz):
        recv(("bh", dz), oneb)
        b_mate(dz, 2)

    def bz(n):
        recv(("bz", n), twob if n < 4 else oneb)
        for r, half in way:
            if n < 3:
                send(("bz", n + 1), "bz", zb(-r * n), zdev[r])
            elif n == 3:
                send(("bz", 4), "bzh", zb(-r * 3, half), zdev[r])
        for dz in (n, -n) if n < 4 else (4,):
            bx_send(dz)

    def az_send(n, dx, r):
        if n < 4:
            send(("az", n, dx), "az", za(-r * (n - 1), dx), zdev[r])
        else:
            send(("az", 4, dx), "azh", za(-r * 3, dx, 0 if r == 1 else 1), zdev[r])

    def az(n, dx):
        recv(("az", n, dx), twoa if n < 4 else onea)
        for r in (1, -1):
            if n < 4:
                az_send(n + 1, dx, r)
        for dz in (n, -n) if n < 4 else (4,):
            a_mate(dz, dx)

    def ax_mid():
        recv(("ax",), twoa)
        for r, half in way:
            send(("ah",), "ah", xa(-r, half), xdev[r])
        for r in (1, -1):
            for dx in (1, -1):
                az_send(1, dx, r)
        for r in (1, -1):
            a_mate(0, r)

    def ax_end():
        recv(("ah",), onea)
        for r in (1, -1):
            az_send(1, 2, r)
        a_mate(0, 2)

    def turn_down(dz):
        zz = (z + dz + NZ) % NZ
        recv(("am", dz), wa.at[0, :, 0])
        dt[:, pl.ds(pl.multiple_of(zz * 256, 256), 256)] = wa[zz, :, :, :, 2 * rest :].reshape(256, FFL).T

    def mates():
        recv(("bm",), wb.at[:, :, 0])

    def begin():
        loaded("kv", kv.at[:, pl.ds(0, TOK)])
        send(("halo",), "halo", kv.at[:, pl.ds(WINDOW, WINDOW)], hdev[-1], kv.at[:, pl.ds(WINDOW + TOK, WINDOW)])
        send(("halo",), "halo", kv.at[:, pl.ds(TOK, WINDOW)], hdev[1], kv.at[:, pl.ds(0, WINDOW)])
        loaded("b", oneb)
        loaded("a", onea)
        for r in (1, -1):
            send(("bz", 1), "bz", zb(0), zdev[r])
            send(("ax",), "ax", xa(0), xdev[r])
        for r in (1, -1):
            az_send(1, 0, r)
        bx_send(0)
        a_mate(0, 0)

    loaded("tab", tab)
    cb = tab[pl.ds(2 * EXT + s, 1), :]
    sb = tab[pl.ds(2 * EXT + nsp + s, 1), :]

    def rotate(rows, value):
        cl, sl = tab[rows, :], tab[pl.ds(EXT + rows.start, rows.size), :]
        cos = cb * cl - sb * sl
        sin = sb * cl + cb * sl
        return value.astype(F32) * cos + mm(value, turn) * sin

    jj = lax.broadcasted_iota(jnp.int32, (128, 128), 0)
    ii = lax.broadcasted_iota(jnp.int32, (128, 128), 1)
    low = (ii % 64) < 32
    turn = (jnp.where(jj == ii - 32, jnp.where(low, 0.0, 1.0), 0.0)
            - jnp.where(jj == ii + 32, jnp.where(low, 1.0, 0.0), 0.0)).astype(BF)
    flip = jnp.where((jj + 64) % 128 == ii, 1.0, 0.0).astype(BF)

    def turn_q():
        loaded("q", q)
        for t in range(4):
            qr[t] = rotate(pl.ds(WINDOW, TOK), q[:, 128 * t : 128 * (t + 1)]).astype(BF)

    def prepare(first, many):
        rows = pl.ds(first, many)
        lane = lax.broadcasted_iota(jnp.int32, (many, 128), 1)
        left = lane < 64
        kr = rotate(rows, kv[0, rows]).astype(BF)
        ks = mm(kr, flip)
        kr = kr.astype(F32)
        vr = kv[1, rows].astype(F32)
        vs = mm(kv[1, rows], flip)
        for i in range(4):
            ksrc, vsrc = ((kr, vr), (ks, vs), (ks, vs), (kr, vr))[i]
            keep = left if i % 2 == 0 else lane >= 64
            kk[i, rows, :] = jnp.where(keep, ksrc, 0.0).astype(BF)
            vv[i, rows, :128] = jnp.where(keep, vsrc, 0.0).astype(BF)

    def prepare_own():
        left = lax.broadcasted_iota(jnp.int32, (EXT, 128), 1) < 64
        one = jnp.where(left, 1.0, 0.0).astype(BF)
        two = jnp.where(left, 0.0, 1.0).astype(BF)
        for i in range(4):
            kk[i, EXT:, :] = jnp.zeros((PAD - EXT, 128), BF)
            vv[i, EXT:, :] = jnp.zeros((PAD - EXT, 256), BF)
            vv[i, :EXT, 128:] = one if i % 2 == 0 else two
        prepare(WINDOW, TOK)

    def prepare_ends():
        recv(("halo",), kv.at[:, pl.ds(0, 2 * WINDOW)])
        prepare(0, WINDOW)
        prepare(WINDOW + TOK, WINDOW)

    def attend(b):
        first = s * TOK + b * BLK
        ri = lax.broadcasted_iota(jnp.int32, (BLK, QW), 0)
        ci = lax.broadcasted_iota(jnp.int32, (BLK, QW), 1)
        lo = jnp.maximum(ri, WINDOW - first)
        hi = jnp.minimum(ri + 2 * WINDOW, nsp * TOK - 1 + WINDOW - first)
        bias[...] = jnp.where((ci >= lo) & (ci <= hi), 0.0, -jnp.inf)
        rows = pl.multiple_of(b * BLK, 32)
        half = lax.broadcasted_iota(jnp.int32, (BLK, 128), 1) < 64

        def tile(t, carry):
            qt = qr[t, pl.ds(rows, BLK), :]
            acc, ends = None, []
            for par in range(2):
                i = (t // 2) * 2 + par
                sc = nt(qt, kk[i, pl.ds(rows, QW), :]) * 0.125 + bias[...]
                snk = sink[2 * t + par]
                top = jnp.maximum(jnp.max(sc, axis=1, keepdims=True), snk)
                prob = jnp.exp(sc - top).astype(BF)
                part = mm(prob, vv[i, pl.ds(rows, QW), :])
                acc = part if acc is None else acc + part
                ends.append(jnp.exp(snk - top))
            den = acc[:, 128:] + jnp.where(half, ends[0], ends[1])
            att[:, pl.ds(pl.multiple_of(t * 128, 128), 128)] = (acc[:, :128] / den).astype(BF)
            return carry

        lax.fori_loop(0, 4, tile, 0, unroll=True)

    UP, LOW = 0, 1
    at_half = {("n", LOW): 0, ("p", UP): 1, ("f", UP): 2, ("f", LOW): 3, ("n", UP): 4, ("p", LOW): 5, ("o", UP): 6, ("o", LOW): 7}
    ahead = {1: "n", -1: "p"}
    back = {1: "p", -1: "n"}
    via = {1: UP, -1: LOW}
    cols_of = [pl.ds(i * (D // SUB), D // SUB) for i in range(SUB)]

    def project(block):
        def cols(n, carry):
            at_n = pl.ds(pl.multiple_of(n * 512, 512), 512)
            done = mm(att[...], ow[:, at_n]).astype(BF)
            for part in (UP, LOW):
                pb1[at_half[block, part], :, at_n] = done[part * HALF : (part + 1) * HALF]
            return carry

        lax.fori_loop(0, 4, cols, 0)

    def rs_far(tag, pb, sbuf):
        for i, cols in enumerate(cols_of):
            for r in (1, -1):
                key = (tag, "s", i) if tag == "r2" else (tag, "s", r, i)
                send(key, tag, pb.at[at_half["f", via[r]], :, cols], ydev[r], sbuf.at[via[r], :, cols])

    def sum_key(tag, part, i):
        return (tag, "f", i if tag == "r2" else part)

    def rs_near(tag, pb, fbuf, r, i):
        part, cols = 1 - via[r], cols_of[i]
        send(sum_key(tag, part, i), tag, pb.at[at_half[ahead[r], part], :, cols], ydev[r], fbuf.at[part, via[r], :, cols])

    def rs_relay(tag, pb, sbuf, fbuf, r, i):
        cols, part = cols_of[i], via[r]
        j = at_half[ahead[r], part]
        if tag == "r1":
            recv((tag, "s", r, i), sbuf.at[part, :, cols])
        pb[j, :, cols] = (pb[j, :, cols].astype(F32) + sbuf[part, :, cols].astype(F32)).astype(BF)
        send(sum_key(tag, part, i), tag, pb.at[j, :, cols], ydev[r], fbuf.at[part, via[r], :, cols])

    def rs_sum(pb, fbuf, part, cols):
        own = pb[at_half["o", part], :, cols].astype(F32)
        return own + fbuf[part, 0, :, cols].astype(F32) + fbuf[part, 1, :, cols].astype(F32)

    ynext = {"f": (y + 2) % NY, "n": (y + 1) % NY, "p": (y + NY - 1) % NY, "o": y}

    def normalise(part):
        rows = pl.ds(part * HALF, HALF)
        recv(sum_key("r1", part, 0), pb1.at[pl.ds(0, 2)])
        total = st[rows, :].astype(F32) + rs_sum(pb1, f1, part, slice(None))
        mixed[rows, :] = total.astype(BF)
        wide = mixed[rows, :].astype(F32)
        scale = lax.rsqrt(jnp.mean(wide * wide, axis=1, keepdims=True) + 1e-06)
        xs[at_half["o", part]] = (wide * scale * gain[...]).astype(BF)

    def g_cols(part):
        return cols_of if part == LOW else [pl.ds(0, D)]

    def g_send(part):
        for i, cols in enumerate(g_cols(part)):
            for r in (1, -1):
                send(("g", part, i), "g", xs.at[at_half["o", part], :, cols], ydev[r], xs.at[at_half[back[r], part], :, cols])

    def g_recv(part, i):
        cols = g_cols(part)[i]
        recv(("g", part, i), xs.at[pl.ds(0, 2), :, cols])
        for r in (1, -1):
            if via[r] == part:
                ref = xs.at[at_half[back[r], part], :, cols]
                send(("gh",), "g", ref, ydev[r], xs.at[at_half["f", part], :, cols])

    def g_far():
        recv(("gh",), xs.at[pl.ds(0, 2)])

    def gate_up(first, count):
        many = count * HALF
        rows = pl.ds(0, many)

        def act(gate, upward):
            return (gate / (1.0 + jnp.exp(-gate)) * upward).astype(BF)

        def cols(n, carry):
            gu = []
            for base in (0, GB):
                w = wb[:, :, :, :, pl.ds(pl.multiple_of(base + n * 256, 256), 256)].reshape(D, 256)
                gu.append(mm(xs[first : first + count].reshape(many, D), w))
            hid[rows, pl.ds(pl.multiple_of(n * 256, 256), 256)] = act(*gu)
            return carry

        gu = mm(xs[first : first + count].reshape(many, D), wa[:, :, :, :, : 2 * rest].reshape(D, 2 * rest))
        hid[rows, GB:] = act(gu[:, :rest], gu[:, rest:])
        lax.fori_loop(0, GB // 256, cols, 0, unroll=True)

    def down(first, count, i):
        many = count * HALF

        def cols(n, carry):
            at_n = pl.ds(pl.multiple_of(i * (D // SUB) + n * 512, 512), 512)
            done = mm(hid[pl.ds(0, many), :], dt[:, at_n]).astype(BF)
            pb2[first : first + count, :, at_n] = done.reshape(count, HALF, 512)
            return carry

        lax.fori_loop(0, D // SUB // 512, cols, 0, unroll=True)

    def near2(i):
        down(0, 2, i)
        for r in (1, -1):
            rs_near("r2", pb2, f2, r, i)

    def far2():
        g_far()
        gate_up(2, 2)
        for i in range(SUB):
            down(2, 2, i)
        rs_far("r2", pb2, s2)

    def own2():
        gate_up(4, 4)
        for i in range(SUB):
            down(4, 4, i)

    def first2():
        mates()
        gate_up(0, 2)

    def near1(r):
        for i in range(SUB):
            rs_near("r1", pb1, f1, r, i)

    def relay2(i):
        recv(("r2", "s", i), s2.at[:, :, cols_of[i]])
        for r in (1, -1):
            rs_relay("r2", pb2, s2, f2, r, i)

    def attend_on(block):
        if block == "o":
            loaded("st", st)
        attend(ynext[block])

    def project_on(block):
        if block == "f":
            loaded("ow", ow)
        project(block)
        if block == "f":
            rs_far("r1", pb1, s1)
        if block == "p":
            near1(-1)

    def norm_on(part):
        normalise(part)
        g_send(part)

    steps = {
        "begin": begin,
        "turn_q": turn_q,
        "prep_own": prepare_own,
        "prepare": prepare_ends,
        "near+": lambda: near1(1),
        "norm_U": lambda: norm_on(UP),
        "norm_L": lambda: norm_on(LOW),
        "gU": lambda: g_recv(UP, 0),
        "gL0": lambda: g_recv(LOW, 0),
        "gL1": lambda: g_recv(LOW, 1),
        "ax_mid": ax_mid,
        "ax_end": ax_end,
        "feed1": first2,
        "near0": lambda: near2(0),
        "near1": lambda: near2(1),
        "feed2": far2,
        "feed3": own2,
        "r2l0": lambda: relay2(0),
        "r2l1": lambda: relay2(1),
        "fin0": lambda: finish(0),
        "fin1": lambda: finish(1),
    }

    def run_steps(name):
        if name in steps:
            return steps[name]()
        head, *rest_of = name.split("_")
        if head == "att":
            return attend_on(rest_of[0])
        if head == "proj":
            return project_on(rest_of[0])
        if head[:2] == "rl":
            return rs_relay("r1", pb1, s1, f1, 1 if head[2] == "+" else -1, int(head[3]))
        numbers = [int(n) for n in rest_of]
        return {"bz": bz, "bm": bx_mid, "be": bx_end, "az": az, "tr": turn_down}[head](*numbers)

    def finish(i):
        cols = cols_of[i]
        recv(("r2", "f", i), pb2.at[pl.ds(0, 2)])
        for part in (UP, LOW):
            rows = pl.ds(part * HALF, HALF)
            out[rows, cols] = mixed[rows, cols].astype(F32) + 0.5 * rs_sum(pb2, f2, part, cols)

    for name in ORDER:
        run_steps(name)

    def drain():
        everything = {
            "halo": kv.at[:, pl.ds(0, 2 * WINDOW)],
            "bz": wb.at[pl.ds(0, 6), 0, 0], "bzh": oneb, "bx": wb.at[:, pl.ds(0, 2), 0], "bh": wb.at[:, 0, 0],
            "bm": wb.at[:, :, 0], "ax": twoa, "ah": onea, "az": wa.at[pl.ds(0, 6), :, 0], "azh": wa.at[0, :, 0],
            "am": wa.at[:, :, 0], "r1": pb1.at[pl.ds(0, 6)], "r2": pb2.at[pl.ds(0, 6)], "g": xs.at[pl.ds(0, 6)],
        }
        for kind, ref in everything.items():
            pltpu.make_async_copy(ref, ref, ssem.at[given[kind]]).wait()

    drain()
    assert len(taken) == NRECV and len(given) == NSEND, (len(taken), len(given))


def local(queries, keys, values, sink, stream, out_weight, norm_gain, gate_weight, up_weight, down_weight):
    hbm = pl.BlockSpec(memory_space=pl.ANY)
    vmem = pl.BlockSpec(memory_space=pltpu.VMEM)
    smem = pl.BlockSpec(memory_space=pltpu.SMEM)
    V = pltpu.VMEM
    done = pl.pallas_call(
        kernel,
        name="layer",
        out_shape=jax.ShapeDtypeStruct((BLK, D), F32),
        in_specs=[hbm, hbm, hbm, smem, hbm, hbm, vmem, hbm, hbm, hbm, hbm],
        out_specs=vmem,
        scratch_shapes=[
            V((NZ, NX, NC, ROWS, CA), BF),
            V((NZ, NX, NC, ROWS, CB), BF),
            V((2 * EXT + 2 * NZ * NX * NC, 128), F32),
            V((TOK, 512), BF),
            V((4, TOK, 128), BF),
            V((2, EXT, 128), BF),
            V((4, PAD, 128), BF),
            V((4, PAD, 256), BF),
            V((512, D), BF),
            V((BLK, D), BF),
            V((BLK, QW), F32),
            V((BLK, 512), BF),
            V((8, HALF, D), BF),
            V((2, HALF, D), BF),
            V((2, 2, HALF, D), BF),
            V((8, HALF, D), BF),
            V((2, HALF, D), BF),
            V((2, 2, HALF, D), BF),
            V((BLK, D), BF),
            V((8, HALF, D), BF),
            V((2 * BLK, FFL), BF),
            V((FFL, D), BF),
            pltpu.SemaphoreType.DMA((7,)),
            pltpu.SemaphoreType.DMA((NSEND,)),
            pltpu.SemaphoreType.DMA((NRECV,)),
        ],
        compiler_params=pltpu.CompilerParams(
            collective_id=0, has_side_effects=True, vmem_limit_bytes=62 * 1024 * 1024
        ),
    )(
        queries, keys, values, sink, stream, out_weight, norm_gain.reshape(1, D),
        gate_weight, up_weight, down_weight.T, jnp.asarray(tables()),
    )
    return done.astype(BF)


def solution(mesh):
    placed = (
        P("sp", "tp"), P("sp", "tp"), P("sp", "tp"), P("tp"), P(("sp", "tp"), None), P("tp", None), P(),
        P("sp", "tp"), P("sp", "tp"), P("tp", "sp"),
    )
    return jax.shard_map(local, mesh=mesh, in_specs=placed, out_specs=P(("sp", "tp"), None), check_vma=False)
```

```python
import jax
import jax.numpy as jnp
import numpy as np
from jax import lax
from jax.experimental import pallas as pl
from jax.experimental.pallas import tpu as pltpu
from jax.sharding import PartitionSpec as P

HEAD = 64
WINDOW = 128
MESH = pl.DeviceIdType.MESH
BF = jnp.bfloat16
F32 = jnp.float32

NZ, NX, NC, NY = 8, 4, 2, 4
ROWS = 32
TOK = 640
BLK = TOK // NY
HALF = BLK // 2
EXT = TOK + 2 * WINDOW
PAD = 3 * BLK + 4 * WINDOW
D = 2048
FFL = 1408
GB = 1280
CB = 2 * GB
CA = 2 * (FFL - GB) + FFL
QW = 512
NRECV = 63
NSEND = 14
ORDER = (
    "begin", "turn_q", "prep_own", "prepare", "att_f", "proj_f", "bz_1", "att_n", "proj_n", "att_p", "az_1_0",
    "proj_p", "ax_mid", "att_o", "rl-0", "proj_o", "bz_2", "bm_1", "rl+0", "bm_0", "az_2_0", "rl+1", "near+", "rl-1",
    "bm_-1", "ax_end", "az_1_1", "tr_0", "az_1_-1", "bm_2", "bz_3", "norm_U", "bm_-2", "az_3_0", "be_1", "az_1_2",
    "be_0", "tr_1", "tr_-1", "be_-1", "az_2_1", "norm_L", "be_2", "az_2_-1", "bz_4", "bm_3", "az_4_0", "az_2_2",
    "gU", "bm_-3", "tr_2", "tr_-2", "az_3_1", "be_-2", "gL0", "az_3_-1", "bm_4", "az_3_2", "gL1", "early1", "az_4_1",
    "be_3", "tr_3", "az_4_-1", "tr_-3", "be_-3", "az_4_2", "be_4", "tr_4", "feed1", "near0", "near1", "feed2",
    "feed3", "r2l0", "r2l1", "fin0", "fin1",
)
SUB = 2


def tables():
    lane = (np.arange(128) % 64) % 32
    freq = 1.0 / 10000.0 ** (2.0 * lane / HEAD)
    near = (np.arange(EXT) - WINDOW)[:, None] * freq[None]
    far = (np.arange(NZ * NX * NC) * TOK)[:, None] * freq[None]
    return np.concatenate([np.cos(near), np.sin(near), np.cos(far), np.sin(far)], 0).astype(np.float32)


def nt(a, b):
    return lax.dot_general(a, b, (((1,), (1,)), ((), ())), preferred_element_type=F32)


def mm(a, b):
    return jnp.dot(a, b, preferred_element_type=F32)


def kernel(
    q_hbm, k_hbm, v_hbm, sink_hbm, st_hbm, ow_hbm, gain_hbm, g_hbm, u_hbm, d_hbm, tab_hbm,
    out,
    wa, wb, tab, q, qr, kv, kk, vv, ow, st, bias, att,
    pb1, s1, f1, pb2, s2, f2, mixed, xs, hid, dt, pre, gain, sink,
    lsem, ssem, rsem,
):
    s = lax.axis_index("sp")
    y = lax.axis_index("tp")
    c = s % NC
    x = (s // NC) % NX
    z = s // (NC * NX)

    def at(zz, xx, cc):
        return ((zz % NZ) * NX + xx % NX) * NC + cc

    ydev = {1: (s, (y + 1) % NY), -1: (s, (y + NY - 1) % NY)}
    xdev = {1: (at(z, x + 1, c), y), -1: (at(z, x + NX - 1, c), y)}
    zdev = {1: (at(z + 1, x, c), y), -1: (at(z + NZ - 1, x, c), y)}
    mate = (at(z, x, 1 - c), y)
    nsp = NZ * NX * NC
    hdev = {1: ((s + 1) % nsp, y), -1: ((s + nsp - 1) % nsp, y)}

    barrier = pltpu.get_barrier_semaphore()
    for dev in (*ydev.values(), *xdev.values(), *zdev.values(), mate, *hdev.values()):
        pl.semaphore_signal(barrier, inc=1, device_id=dev, device_id_type=MESH)

    loads = {}

    def load(name, src, dst):
        i = loads.setdefault(name, len(loads))
        pltpu.make_async_copy(src, dst, lsem.at[i]).start()

    def loaded(name, ref):
        pltpu.make_async_copy(ref, ref, lsem.at[loads[name]]).wait()

    rest = FFL - GB
    load("kv", k_hbm, kv.at[0, pl.ds(WINDOW, TOK)])
    load("kv", v_hbm, kv.at[1, pl.ds(WINDOW, TOK)])
    load("b", g_hbm.at[:, pl.ds(0, GB)], wb.at[z, x, c, :, pl.ds(0, GB)])
    load("b", u_hbm.at[:, pl.ds(0, GB)], wb.at[z, x, c, :, pl.ds(GB, GB)])
    load("a", d_hbm, wa.at[z, x, c, :, pl.ds(2 * rest, FFL)])
    load("a", g_hbm.at[:, pl.ds(GB, rest)], wa.at[z, x, c, :, pl.ds(0, rest)])
    load("a", u_hbm.at[:, pl.ds(GB, rest)], wa.at[z, x, c, :, pl.ds(rest, rest)])
    load("tab", tab_hbm, tab)
    load("q", q_hbm, q)
    load("ow", ow_hbm, ow)
    load("st", st_hbm, st)
    load("gain", gain_hbm, gain)
    load("sink", sink_hbm, sink)

    def greet():
        pl.semaphore_wait(barrier, 9)

    greet()

    taken, given = {}, {}

    def send(key, kind, ref, dev, dst=None):
        i = taken.setdefault(key, len(taken))
        k = given.setdefault(kind, len(given))
        pltpu.make_async_remote_copy(
            src_ref=ref, dst_ref=ref if dst is None else dst, send_sem=ssem.at[k], recv_sem=rsem.at[i],
            device_id=dev, device_id_type=MESH,
        ).start()

    def recv(key, ref):
        i = taken.setdefault(key, len(taken))
        pltpu.make_async_copy(ref, ref, rsem.at[i]).wait()

    def zb(dz, half=None):
        ref = wb.at[(z + dz + NZ) % NZ, x, c]
        return ref if half is None else ref.at[pl.ds(16 * half, 16)]

    def xb(dz, dx, half=None):
        ref = wb.at[(z + dz + NZ) % NZ, (x + dx + NX) % NX, c]
        return ref if half is None else ref.at[pl.ds(16 * half, 16)]

    def za(dz, dx, half=None):
        ref = wa.at[(z + dz + NZ) % NZ, (x + dx + NX) % NX, c]
        return ref if half is None else ref.at[pl.ds(16 * half, 16)]

    def xa(dx, half=None):
        ref = wa.at[z, (x + dx + NX) % NX, c]
        return ref if half is None else ref.at[pl.ds(16 * half, 16)]

    oneb, onea = wb.at[0, 0, 0], wa.at[0, 0, 0]
    twob, twoa = wb.at[pl.ds(0, 2), 0, 0], wa.at[pl.ds(0, 2), 0, 0]
    way = ((1, 0), (-1, 1))

    def b_mate(dz, dx):
        send(("bm", abs(dz) > 2), "bm", xb(dz, dx), mate)

    def a_mate(dz, dx):
        send(("am", dz), "am", za(dz, dx), mate)

    def bx_send(dz):
        for r in (1, -1):
            send(("bx", dz), "bx", xb(dz, 0), xdev[r])
        b_mate(dz, 0)

    def bx_mid(dz):
        recv(("bx", dz), twob)
        for r, half in way:
            send(("bh", dz), "bh", xb(dz, -r, half), xdev[r])
        for r in (1, -1):
            b_mate(dz, r)

    def bx_end(dz):
        recv(("bh", dz), oneb)
        b_mate(dz, 2)

    def bz(n):
        recv(("bz", n), twob if n < 4 else oneb)
        for r, half in way:
            if n < 3:
                send(("bz", n + 1), "bz", zb(-r * n), zdev[r])
            elif n == 3:
                send(("bz", 4), "bzh", zb(-r * 3, half), zdev[r])
        for dz in (n, -n) if n < 4 else (4,):
            bx_send(dz)

    def az_send(n, dx, r):
        if n < 4:
            send(("az", n, dx), "az", za(-r * (n - 1), dx), zdev[r])
        else:
            send(("az", 4, dx), "azh", za(-r * 3, dx, 0 if r == 1 else 1), zdev[r])

    def az(n, dx):
        recv(("az", n, dx), twoa if n < 4 else onea)
        for r in (1, -1):
            if n < 4:
                az_send(n + 1, dx, r)
        for dz in (n, -n) if n < 4 else (4,):
            a_mate(dz, dx)

    def ax_mid():
        recv(("ax",), twoa)
        for r, half in way:
            send(("ah",), "ah", xa(-r, half), xdev[r])
        for r in (1, -1):
            for dx in (1, -1):
                az_send(1, dx, r)
        for r in (1, -1):
            a_mate(0, r)

    def ax_end():
        recv(("ah",), onea)
        for r in (1, -1):
            az_send(1, 2, r)
        a_mate(0, 2)

    def turn_down(dz):
        zz = (z + dz + NZ) % NZ
        recv(("am", dz), wa.at[0, :, 0])
        dt[:, pl.ds(pl.multiple_of(zz * 256, 256), 256)] = wa[zz, :, :, :, 2 * rest :].reshape(256, FFL).T

    def mates(last):
        recv(("bm", last), wb.at[pl.ds(0, 3 if last else 5), :, 0])

    def begin():
        loaded("kv", kv.at[:, pl.ds(0, TOK)])
        send(("halo",), "halo", kv.at[:, pl.ds(WINDOW, WINDOW)], hdev[-1], kv.at[:, pl.ds(WINDOW + TOK, WINDOW)])
        send(("halo",), "halo", kv.at[:, pl.ds(TOK, WINDOW)], hdev[1], kv.at[:, pl.ds(0, WINDOW)])
        loaded("b", oneb)
        loaded("a", onea)
        for r in (1, -1):
            send(("bz", 1), "bz", zb(0), zdev[r])
            send(("ax",), "ax", xa(0), xdev[r])
        for r in (1, -1):
            az_send(1, 0, r)
        bx_send(0)
        a_mate(0, 0)

    loaded("tab", tab)
    cb = tab[pl.ds(2 * EXT + s, 1), :]
    sb = tab[pl.ds(2 * EXT + nsp + s, 1), :]

    def rotate(rows, value):
        cl, sl = tab[rows, :], tab[pl.ds(EXT + rows.start, rows.size), :]
        cos = cb * cl - sb * sl
        sin = sb * cl + cb * sl
        return value.astype(F32) * cos + mm(value, turn) * sin

    jj = lax.broadcasted_iota(jnp.int32, (128, 128), 0)
    ii = lax.broadcasted_iota(jnp.int32, (128, 128), 1)
    low = (ii % 64) < 32
    turn = (jnp.where(jj == ii - 32, jnp.where(low, 0.0, 1.0), 0.0)
            - jnp.where(jj == ii + 32, jnp.where(low, 1.0, 0.0), 0.0)).astype(BF)
    flip = jnp.where((jj + 64) % 128 == ii, 1.0, 0.0).astype(BF)

    def turn_q():
        loaded("q", q)
        for t in range(4):
            qr[t] = rotate(pl.ds(WINDOW, TOK), q[:, 128 * t : 128 * (t + 1)]).astype(BF)

    def prepare(first, many):
        rows = pl.ds(first, many)
        lane = lax.broadcasted_iota(jnp.int32, (many, 128), 1)
        left = lane < 64
        kr = rotate(rows, kv[0, rows]).astype(BF)
        ks = mm(kr, flip)
        kr = kr.astype(F32)
        vr = kv[1, rows].astype(F32)
        vs = mm(kv[1, rows], flip)
        for i in range(4):
            ksrc, vsrc = ((kr, vr), (ks, vs), (ks, vs), (kr, vr))[i]
            keep = left if i % 2 == 0 else lane >= 64
            kk[i, rows, :] = jnp.where(keep, ksrc, 0.0).astype(BF)
            vv[i, rows, :128] = jnp.where(keep, vsrc, 0.0).astype(BF)

    def prepare_own():
        left = lax.broadcasted_iota(jnp.int32, (EXT, 128), 1) < 64
        one = jnp.where(left, 1.0, 0.0).astype(BF)
        two = jnp.where(left, 0.0, 1.0).astype(BF)
        for i in range(4):
            kk[i, EXT:, :] = jnp.zeros((PAD - EXT, 128), BF)
            vv[i, EXT:, :] = jnp.zeros((PAD - EXT, 256), BF)
            vv[i, :EXT, 128:] = one if i % 2 == 0 else two
        prepare(WINDOW, TOK)

    def prepare_ends():
        recv(("halo",), kv.at[:, pl.ds(0, 2 * WINDOW)])
        prepare(0, WINDOW)
        prepare(WINDOW + TOK, WINDOW)

    def attend(b):
        first = s * TOK + b * BLK
        ri = lax.broadcasted_iota(jnp.int32, (BLK, QW), 0)
        ci = lax.broadcasted_iota(jnp.int32, (BLK, QW), 1)
        lo = jnp.maximum(ri, WINDOW - first)
        hi = jnp.minimum(ri + 2 * WINDOW, nsp * TOK - 1 + WINDOW - first)
        bias[...] = jnp.where((ci >= lo) & (ci <= hi), 0.0, -jnp.inf)
        rows = pl.multiple_of(b * BLK, 32)
        half = lax.broadcasted_iota(jnp.int32, (BLK, 128), 1) < 64

        def tile(t, carry):
            qt = qr[t, pl.ds(rows, BLK), :]
            acc, ends = None, []
            for par in range(2):
                i = (t // 2) * 2 + par
                sc = nt(qt, kk[i, pl.ds(rows, QW), :]) * 0.125 + bias[...]
                snk = sink[2 * t + par]
                top = jnp.maximum(jnp.max(sc, axis=1, keepdims=True), snk)
                prob = jnp.exp(sc - top).astype(BF)
                part = mm(prob, vv[i, pl.ds(rows, QW), :])
                acc = part if acc is None else acc + part
                ends.append(jnp.exp(snk - top))
            den = acc[:, 128:] + jnp.where(half, ends[0], ends[1])
            att[:, pl.ds(pl.multiple_of(t * 128, 128), 128)] = (acc[:, :128] / den).astype(BF)
            return carry

        lax.fori_loop(0, 4, tile, 0, unroll=True)

    UP, LOW = 0, 1
    at_half = {("n", LOW): 0, ("p", UP): 1, ("f", UP): 2, ("f", LOW): 3, ("n", UP): 4, ("p", LOW): 5, ("o", UP): 6, ("o", LOW): 7}
    ahead = {1: "n", -1: "p"}
    back = {1: "p", -1: "n"}
    via = {1: UP, -1: LOW}
    cols_of = [pl.ds(i * (D // SUB), D // SUB) for i in range(SUB)]

    def project(block):
        def cols(n, carry):
            at_n = pl.ds(pl.multiple_of(n * 512, 512), 512)
            done = mm(att[...], ow[:, at_n]).astype(BF)
            for part in (UP, LOW):
                pb1[at_half[block, part], :, at_n] = done[part * HALF : (part + 1) * HALF]
            return carry

        lax.fori_loop(0, 4, cols, 0)

    def rs_far(tag, pb, sbuf):
        for i, cols in enumerate(cols_of):
            for r in (1, -1):
                key = (tag, "s", i) if tag == "r2" else (tag, "s", r, i)
                send(key, tag, pb.at[at_half["f", via[r]], :, cols], ydev[r], sbuf.at[via[r], :, cols])

    def sum_key(tag, part, i):
        return (tag, "f", i if tag == "r2" else part)

    def rs_near(tag, pb, fbuf, r, i):
        part, cols = 1 - via[r], cols_of[i]
        send(sum_key(tag, part, i), tag, pb.at[at_half[ahead[r], part], :, cols], ydev[r], fbuf.at[part, via[r], :, cols])

    def rs_relay(tag, pb, sbuf, fbuf, r, i):
        cols, part = cols_of[i], via[r]
        j = at_half[ahead[r], part]
        if tag == "r1":
            recv((tag, "s", r, i), sbuf.at[part, :, cols])
        pb[j, :, cols] = (pb[j, :, cols].astype(F32) + sbuf[part, :, cols].astype(F32)).astype(BF)
        send(sum_key(tag, part, i), tag, pb.at[j, :, cols], ydev[r], fbuf.at[part, via[r], :, cols])

    def rs_sum(pb, fbuf, part, cols):
        own = pb[at_half["o", part], :, cols].astype(F32)
        return own + fbuf[part, 0, :, cols].astype(F32) + fbuf[part, 1, :, cols].astype(F32)

    ynext = {"f": (y + 2) % NY, "n": (y + 1) % NY, "p": (y + NY - 1) % NY, "o": y}

    def normalise(part):
        rows = pl.ds(part * HALF, HALF)
        recv(sum_key("r1", part, 0), pb1.at[pl.ds(0, 2)])
        total = st[rows, :].astype(F32) + rs_sum(pb1, f1, part, slice(None))
        mixed[rows, :] = total.astype(BF)
        wide = mixed[rows, :].astype(F32)
        scale = lax.rsqrt(jnp.mean(wide * wide, axis=1, keepdims=True) + 1e-06)
        xs[at_half["o", part]] = (wide * scale * gain[...]).astype(BF)

    def g_cols(part):
        return cols_of if part == LOW else [pl.ds(0, D)]

    def g_send(part):
        for i, cols in enumerate(g_cols(part)):
            for r in (1, -1):
                send(("g", part, i), "g", xs.at[at_half["o", part], :, cols], ydev[r], xs.at[at_half[back[r], part], :, cols])

    def g_recv(part, i):
        cols = g_cols(part)[i]
        recv(("g", part, i), xs.at[pl.ds(0, 2), :, cols])
        for r in (1, -1):
            if via[r] == part:
                ref = xs.at[at_half[back[r], part], :, cols]
                send(("gh",), "g", ref, ydev[r], xs.at[at_half["f", part], :, cols])

    def g_far():
        recv(("gh",), xs.at[pl.ds(0, 2)])

    def gate_up(first, count):
        many = count * HALF
        rows = pl.ds(0, many)

        def act(gate, upward):
            return (gate / (1.0 + jnp.exp(-gate)) * upward).astype(BF)

        def cols(n, carry):
            gu = []
            for base in (0, GB):
                w = wb[:, :, :, :, pl.ds(pl.multiple_of(base + n * 256, 256), 256)].reshape(D, 256)
                gu.append(mm(xs[first : first + count].reshape(many, D), w))
            hid[rows, pl.ds(pl.multiple_of(n * 256, 256), 256)] = act(*gu)
            return carry

        gu = mm(xs[first : first + count].reshape(many, D), wa[:, :, :, :, : 2 * rest].reshape(D, 2 * rest))
        hid[rows, GB:] = act(gu[:, :rest], gu[:, rest:])
        lax.fori_loop(0, GB // 256, cols, 0, unroll=True)

    def over(n, dz):
        zz = (z + dz + NZ) % NZ
        act = xs[0:2, :, pl.ds(pl.multiple_of(zz * 256, 256), 256)].reshape(BLK, 256)
        if n < CB // 256:
            w = wb[zz, :, :, :, 256 * n : 256 * (n + 1)]
        else:
            w = wa[zz, :, :, :, : 2 * rest]
        return mm(act, w.reshape(256, 256))

    def early():
        mates(False)
        for n in range(CB // 256 + 1):
            acc = over(n, 0)
            for dz in (1, -1, 2, -2):
                acc = acc + over(n, dz)
            pre[n] = acc

    def late():
        mates(True)
        parts_of = GB // 256

        def total(n):
            return pre[n] + over(n, 3) + over(n, -3) + over(n, 4)

        def act(gate, upward):
            return (gate / (1.0 + jnp.exp(-gate)) * upward).astype(BF)

        for n in range(parts_of):
            hid[:BLK, 256 * n : 256 * (n + 1)] = act(total(n), total(parts_of + n))
        gu = total(2 * parts_of)
        hid[:BLK, GB:] = act(gu[:, :rest], gu[:, rest:])

    def down(first, count, i):
        many = count * HALF

        def cols(n, carry):
            at_n = pl.ds(pl.multiple_of(i * (D // SUB) + n * 512, 512), 512)
            done = mm(hid[pl.ds(0, many), :], dt[:, at_n]).astype(BF)
            pb2[first : first + count, :, at_n] = done.reshape(count, HALF, 512)
            return carry

        lax.fori_loop(0, D // SUB // 512, cols, 0, unroll=True)

    def near2(i):
        down(0, 2, i)
        for r in (1, -1):
            rs_near("r2", pb2, f2, r, i)

    def far2():
        g_far()
        gate_up(2, 2)
        for i in range(SUB):
            down(2, 2, i)
        rs_far("r2", pb2, s2)

    def own2():
        gate_up(4, 4)
        for i in range(SUB):
            down(4, 4, i)

    def near1(r):
        for i in range(SUB):
            rs_near("r1", pb1, f1, r, i)

    def relay2(i):
        recv(("r2", "s", i), s2.at[:, :, cols_of[i]])
        for r in (1, -1):
            rs_relay("r2", pb2, s2, f2, r, i)

    def attend_on(block):
        if block == "f":
            loaded("sink", sink)
        if block == "o":
            loaded("st", st)
            loaded("gain", gain)
        attend(ynext[block])

    def project_on(block):
        if block == "f":
            loaded("ow", ow)
        project(block)
        if block == "f":
            rs_far("r1", pb1, s1)
        if block == "p":
            near1(-1)

    def norm_on(part):
        normalise(part)
        g_send(part)

    steps = {
        "begin": begin,
        "turn_q": turn_q,
        "prep_own": prepare_own,
        "prepare": prepare_ends,
        "near+": lambda: near1(1),
        "norm_U": lambda: norm_on(UP),
        "norm_L": lambda: norm_on(LOW),
        "gU": lambda: g_recv(UP, 0),
        "gL0": lambda: g_recv(LOW, 0),
        "gL1": lambda: g_recv(LOW, 1),
        "ax_mid": ax_mid,
        "ax_end": ax_end,
        "early1": early,
        "feed1": late,
        "near0": lambda: near2(0),
        "near1": lambda: near2(1),
        "feed2": far2,
        "feed3": own2,
        "r2l0": lambda: relay2(0),
        "r2l1": lambda: relay2(1),
        "fin0": lambda: finish(0),
        "fin1": lambda: finish(1),
    }

    def run_steps(name):
        if name in steps:
            return steps[name]()
        head, *rest_of = name.split("_")
        if head == "att":
            return attend_on(rest_of[0])
        if head == "proj":
            return project_on(rest_of[0])
        if head[:2] == "rl":
            return rs_relay("r1", pb1, s1, f1, 1 if head[2] == "+" else -1, int(head[3]))
        numbers = [int(n) for n in rest_of]
        return {"bz": bz, "bm": bx_mid, "be": bx_end, "az": az, "tr": turn_down}[head](*numbers)

    def finish(i):
        cols = cols_of[i]
        recv(("r2", "f", i), pb2.at[pl.ds(0, 2)])
        for part in (UP, LOW):
            rows = pl.ds(part * HALF, HALF)
            out[rows, cols] = (mixed[rows, cols].astype(F32) + 0.5 * rs_sum(pb2, f2, part, cols)).astype(BF)

    for name in ORDER:
        run_steps(name)

    def drain():
        everything = {
            "halo": kv.at[:, pl.ds(0, 2 * WINDOW)],
            "bz": wb.at[pl.ds(0, 6), 0, 0], "bzh": oneb, "bx": wb.at[:, pl.ds(0, 2), 0], "bh": wb.at[:, 0, 0],
            "bm": wb.at[:, :, 0], "ax": twoa, "ah": onea, "az": wa.at[pl.ds(0, 6), :, 0], "azh": wa.at[0, :, 0],
            "am": wa.at[:, :, 0], "r1": pb1.at[pl.ds(0, 6)], "r2": pb2.at[pl.ds(0, 6)], "g": xs.at[pl.ds(0, 6)],
        }
        for kind, ref in everything.items():
            pltpu.make_async_copy(ref, ref, ssem.at[given[kind]]).wait()

    drain()
    assert len(taken) == NRECV and len(given) == NSEND, (len(taken), len(given))


def local(queries, keys, values, sink, stream, out_weight, norm_gain, gate_weight, up_weight, down_weight):
    hbm = pl.BlockSpec(memory_space=pltpu.HBM)
    vmem = pl.BlockSpec(memory_space=pltpu.VMEM)
    V = pltpu.VMEM
    done = pl.pallas_call(
        kernel,
        name="layer",
        out_shape=jax.ShapeDtypeStruct((BLK, D), BF),
        in_specs=[hbm] * 11,
        out_specs=vmem,
        scratch_shapes=[
            V((NZ, NX, NC, ROWS, CA), BF),
            V((NZ, NX, NC, ROWS, CB), BF),
            V((2 * EXT + 2 * NZ * NX * NC, 128), F32),
            V((TOK, 512), BF),
            V((4, TOK, 128), BF),
            V((2, EXT, 128), BF),
            V((4, PAD, 128), BF),
            V((4, PAD, 256), BF),
            V((512, D), BF),
            V((BLK, D), BF),
            V((BLK, QW), F32),
            V((BLK, 512), BF),
            V((8, HALF, D), BF),
            V((2, HALF, D), BF),
            V((2, 2, HALF, D), BF),
            V((8, HALF, D), BF),
            V((2, HALF, D), BF),
            V((2, 2, HALF, D), BF),
            V((BLK, D), BF),
            V((8, HALF, D), BF),
            V((2 * BLK, FFL), BF),
            V((FFL, D), BF),
            V((CB // 256 + 1, BLK, 256), F32),
            V((1, D), F32),
            pltpu.SMEM((8,), F32),
            pltpu.SemaphoreType.DMA((9,)),
            pltpu.SemaphoreType.DMA((NSEND,)),
            pltpu.SemaphoreType.DMA((NRECV,)),
        ],
        compiler_params=pltpu.CompilerParams(
            collective_id=0, has_side_effects=True, vmem_limit_bytes=62 * 1024 * 1024
        ),
    )(
        queries, keys, values, sink, stream, out_weight, norm_gain.reshape(1, D),
        gate_weight, up_weight, down_weight.T, jnp.asarray(tables()),
    )
    return done


def solution(mesh):
    placed = (
        P("sp", "tp"), P("sp", "tp"), P("sp", "tp"), P("tp"), P(("sp", "tp"), None), P("tp", None), P(),
        P("sp", "tp"), P("sp", "tp"), P("tp", "sp"),
    )
    return jax.shard_map(local, mesh=mesh, in_specs=placed, out_specs=P(("sp", "tp"), None), check_vma=False)
```

```python
import jax
import jax.numpy as jnp
import numpy as np
from jax import lax
from jax.experimental import pallas as pl
from jax.experimental.pallas import tpu as pltpu
from jax.sharding import PartitionSpec as P

HEAD = 64
WINDOW = 128
MESH = pl.DeviceIdType.MESH
BF = jnp.bfloat16
F32 = jnp.float32

NZ, NX, NC, NY = 8, 4, 2, 4
ROWS = 32
TOK = 640
BLK = TOK // NY
HALF = BLK // 2
EXT = TOK + 2 * WINDOW
PAD = 3 * BLK + 4 * WINDOW
D = 2048
FFL = 1408
GB = 1280
CB = 2 * GB
CA = 2 * (FFL - GB) + FFL
QW = 512
NRECV = 68
NSEND = 14
ORDER = (
    "begin", "turn_q", "prep_own", "prepare", "att_f", "proj_f", "bz_1", "att_n", "proj_n", "att_p", "az_1_0",
    "ax_mid", "proj_p", "att_o", "proj_o", "rl+0", "bm_1", "bz_2", "rl-0", "bm_0", "az_2_0", "rl+1", "near+", "rl-1",
    "bm_-1", "ax_end", "az_1_1", "tr_0", "be_1", "az_1_-1", "bm_2", "bz_3", "norm_U", "az_3_0", "bm_-2", "az_1_2",
    "be_0", "tr_1", "tr_-1", "be_-1", "az_2_1", "norm_L", "be_2", "az_2_-1", "bz_4", "bm_3", "az_4_0", "gU",
    "az_2_2", "bm_-3", "tr_2", "tr_-2", "az_3_1", "be_-2", "gL0", "az_3_-1", "bm_4", "az_3_2", "gL1", "early1",
    "tr_3", "be_3", "az_4_1", "tr_-3", "az_4_-1", "be_-3", "az_4_2", "early2", "be_4", "tr_4", "feed1", "near0",
    "near1", "near2", "near3", "feed2", "feed3", "r2l0", "r2l1", "r2l2", "r2l3", "fin0", "fin1", "fin2", "fin3",
)
SUB = {"r1": 2, "r2": 4}


def tables():
    lane = (np.arange(128) % 64) % 32
    freq = 1.0 / 10000.0 ** (2.0 * lane / HEAD)
    near = (np.arange(EXT) - WINDOW)[:, None] * freq[None]
    far = (np.arange(NZ * NX * NC) * TOK)[:, None] * freq[None]
    return np.concatenate([np.cos(near), np.sin(near), np.cos(far), np.sin(far)], 0).astype(np.float32)


def nt(a, b):
    return lax.dot_general(a, b, (((1,), (1,)), ((), ())), preferred_element_type=F32)


def mm(a, b):
    return jnp.dot(a, b, preferred_element_type=F32)


def kernel(
    q_hbm, k_hbm, v_hbm, sink_hbm, st_hbm, ow_hbm, gain_hbm, g_hbm, u_hbm, d_hbm, tab_hbm,
    out,
    wa, wb, tab, q, qr, kv, kk, vv, ow, st, bias, att,
    pb1, s1, f1, pb2, s2, f2, mixed, xs, hid, dt, pre, gain, sink, res,
    lsem, ssem, rsem, osem,
):
    s = lax.axis_index("sp")
    y = lax.axis_index("tp")
    c = s % NC
    x = (s // NC) % NX
    z = s // (NC * NX)

    def at(zz, xx, cc):
        return ((zz % NZ) * NX + xx % NX) * NC + cc

    ydev = {1: (s, (y + 1) % NY), -1: (s, (y + NY - 1) % NY)}
    xdev = {1: (at(z, x + 1, c), y), -1: (at(z, x + NX - 1, c), y)}
    zdev = {1: (at(z + 1, x, c), y), -1: (at(z + NZ - 1, x, c), y)}
    mate = (at(z, x, 1 - c), y)
    nsp = NZ * NX * NC
    hdev = {1: ((s + 1) % nsp, y), -1: ((s + nsp - 1) % nsp, y)}

    barrier = pltpu.get_barrier_semaphore()
    for dev in (*ydev.values(), *xdev.values(), *zdev.values(), mate, *hdev.values()):
        pl.semaphore_signal(barrier, inc=1, device_id=dev, device_id_type=MESH)

    loads = {}

    def load(name, src, dst):
        i = loads.setdefault(name, len(loads))
        pltpu.make_async_copy(src, dst, lsem.at[i]).start()

    def loaded(name, ref):
        pltpu.make_async_copy(ref, ref, lsem.at[loads[name]]).wait()

    rest = FFL - GB
    load("kv", k_hbm, kv.at[0, pl.ds(WINDOW, TOK)])
    load("kv", v_hbm, kv.at[1, pl.ds(WINDOW, TOK)])
    load("b", g_hbm.at[:, pl.ds(0, GB)], wb.at[z, x, c, :, pl.ds(0, GB)])
    load("b", u_hbm.at[:, pl.ds(0, GB)], wb.at[z, x, c, :, pl.ds(GB, GB)])
    load("a", d_hbm, wa.at[z, x, c, :, pl.ds(2 * rest, FFL)])
    load("a", g_hbm.at[:, pl.ds(GB, rest)], wa.at[z, x, c, :, pl.ds(0, rest)])
    load("a", u_hbm.at[:, pl.ds(GB, rest)], wa.at[z, x, c, :, pl.ds(rest, rest)])
    load("tab", tab_hbm, tab)
    load("q", q_hbm, q)
    load("ow", ow_hbm, ow)
    load("st", st_hbm, st)
    load("gain", gain_hbm, gain)
    load("sink", sink_hbm, sink)

    def greet():
        pl.semaphore_wait(barrier, 9)

    greet()

    taken, given = {}, {}

    def send(key, kind, ref, dev, dst=None):
        i = taken.setdefault(key, len(taken))
        k = given.setdefault(kind, len(given))
        pltpu.make_async_remote_copy(
            src_ref=ref, dst_ref=ref if dst is None else dst, send_sem=ssem.at[k], recv_sem=rsem.at[i],
            device_id=dev, device_id_type=MESH,
        ).start()

    def recv(key, ref):
        i = taken.setdefault(key, len(taken))
        pltpu.make_async_copy(ref, ref, rsem.at[i]).wait()

    def zb(dz, half=None):
        ref = wb.at[(z + dz + NZ) % NZ, x, c]
        return ref if half is None else ref.at[pl.ds(16 * half, 16)]

    def xb(dz, dx, half=None):
        ref = wb.at[(z + dz + NZ) % NZ, (x + dx + NX) % NX, c]
        return ref if half is None else ref.at[pl.ds(16 * half, 16)]

    def za(dz, dx, half=None):
        ref = wa.at[(z + dz + NZ) % NZ, (x + dx + NX) % NX, c]
        return ref if half is None else ref.at[pl.ds(16 * half, 16)]

    def xa(dx, half=None):
        ref = wa.at[z, (x + dx + NX) % NX, c]
        return ref if half is None else ref.at[pl.ds(16 * half, 16)]

    oneb, onea = wb.at[0, 0, 0], wa.at[0, 0, 0]
    twob, twoa = wb.at[pl.ds(0, 2), 0, 0], wa.at[pl.ds(0, 2), 0, 0]
    way = ((1, 0), (-1, 1))

    def b_mate(dz, dx):
        send(("bm", max(abs(dz), 2)), "bm", xb(dz, dx), mate)

    def a_mate(dz, dx):
        send(("am", dz), "am", za(dz, dx), mate)

    def bx_send(dz):
        for r in (1, -1):
            send(("bx", dz), "bx", xb(dz, 0), xdev[r])
        b_mate(dz, 0)

    def bx_mid(dz):
        recv(("bx", dz), twob)
        for r, half in way:
            send(("bh", dz), "bh", xb(dz, -r, half), xdev[r])
        for r in (1, -1):
            b_mate(dz, r)

    def bx_end(dz):
        recv(("bh", dz), oneb)
        b_mate(dz, 2)

    def bz(n):
        recv(("bz", n), twob if n < 4 else oneb)
        for r, half in way:
            if n < 3:
                send(("bz", n + 1), "bz", zb(-r * n), zdev[r])
            elif n == 3:
                send(("bz", 4), "bzh", zb(-r * 3, half), zdev[r])
        for dz in (n, -n) if n < 4 else (4,):
            bx_send(dz)

    def az_send(n, dx, r):
        if n < 4:
            send(("az", n, dx), "az", za(-r * (n - 1), dx), zdev[r])
        else:
            send(("az", 4, dx), "azh", za(-r * 3, dx, 0 if r == 1 else 1), zdev[r])

    def az(n, dx):
        recv(("az", n, dx), twoa if n < 4 else onea)
        for r in (1, -1):
            if n < 4:
                az_send(n + 1, dx, r)
        for dz in (n, -n) if n < 4 else (4,):
            a_mate(dz, dx)

    def ax_mid():
        recv(("ax",), twoa)
        for r, half in way:
            send(("ah",), "ah", xa(-r, half), xdev[r])
        for r in (1, -1):
            for dx in (1, -1):
                az_send(1, dx, r)
        for r in (1, -1):
            a_mate(0, r)

    def ax_end():
        recv(("ah",), onea)
        for r in (1, -1):
            az_send(1, 2, r)
        a_mate(0, 2)

    def turn_down(dz):
        zz = (z + dz + NZ) % NZ
        recv(("am", dz), wa.at[0, :, 0])
        dt[:, pl.ds(pl.multiple_of(zz * 256, 256), 256)] = wa[zz, :, :, :, 2 * rest :].reshape(256, FFL).T

    def mates(n):
        recv(("bm", n), wb.at[pl.ds(0, {2: 5, 3: 2, 4: 1}[n]), :, 0])

    def begin():
        loaded("kv", kv.at[:, pl.ds(0, TOK)])
        send(("halo",), "halo", kv.at[:, pl.ds(WINDOW, WINDOW)], hdev[-1], kv.at[:, pl.ds(WINDOW + TOK, WINDOW)])
        send(("halo",), "halo", kv.at[:, pl.ds(TOK, WINDOW)], hdev[1], kv.at[:, pl.ds(0, WINDOW)])
        loaded("b", oneb)
        loaded("a", onea)
        for r in (1, -1):
            send(("bz", 1), "bz", zb(0), zdev[r])
            send(("ax",), "ax", xa(0), xdev[r])
        for r in (1, -1):
            az_send(1, 0, r)
        bx_send(0)
        a_mate(0, 0)

    loaded("tab", tab)
    cb = tab[pl.ds(2 * EXT + s, 1), :]
    sb = tab[pl.ds(2 * EXT + nsp + s, 1), :]

    def rotate(rows, value):
        cl, sl = tab[rows, :], tab[pl.ds(EXT + rows.start, rows.size), :]
        cos = cb * cl - sb * sl
        sin = sb * cl + cb * sl
        return value.astype(F32) * cos + mm(value, turn) * sin

    jj = lax.broadcasted_iota(jnp.int32, (128, 128), 0)
    ii = lax.broadcasted_iota(jnp.int32, (128, 128), 1)
    low = (ii % 64) < 32
    turn = (jnp.where(jj == ii - 32, jnp.where(low, 0.0, 1.0), 0.0)
            - jnp.where(jj == ii + 32, jnp.where(low, 1.0, 0.0), 0.0)).astype(BF)
    flip = jnp.where((jj + 64) % 128 == ii, 1.0, 0.0).astype(BF)

    def turn_q():
        loaded("q", q)
        for t in range(4):
            qr[t] = rotate(pl.ds(WINDOW, TOK), q[:, 128 * t : 128 * (t + 1)]).astype(BF)

    def prepare(first, many):
        rows = pl.ds(first, many)
        lane = lax.broadcasted_iota(jnp.int32, (many, 128), 1)
        left = lane < 64
        kr = rotate(rows, kv[0, rows]).astype(BF)
        ks = mm(kr, flip)
        kr = kr.astype(F32)
        vr = kv[1, rows].astype(F32)
        vs = mm(kv[1, rows], flip)
        for i in range(4):
            ksrc, vsrc = ((kr, vr), (ks, vs), (ks, vs), (kr, vr))[i]
            keep = left if i % 2 == 0 else lane >= 64
            kk[i, rows, :] = jnp.where(keep, ksrc, 0.0).astype(BF)
            vv[i, rows, :128] = jnp.where(keep, vsrc, 0.0).astype(BF)

    def prepare_own():
        left = lax.broadcasted_iota(jnp.int32, (EXT, 128), 1) < 64
        one = jnp.where(left, 1.0, 0.0).astype(BF)
        two = jnp.where(left, 0.0, 1.0).astype(BF)
        for i in range(4):
            kk[i, EXT:, :] = jnp.zeros((PAD - EXT, 128), BF)
            vv[i, EXT:, :] = jnp.zeros((PAD - EXT, 256), BF)
            vv[i, :EXT, 128:] = one if i % 2 == 0 else two
        prepare(WINDOW, TOK)

    def prepare_ends():
        recv(("halo",), kv.at[:, pl.ds(0, 2 * WINDOW)])
        prepare(0, WINDOW)
        prepare(WINDOW + TOK, WINDOW)

    def attend(b):
        first = s * TOK + b * BLK
        ri = lax.broadcasted_iota(jnp.int32, (BLK, QW), 0)
        ci = lax.broadcasted_iota(jnp.int32, (BLK, QW), 1)
        lo = jnp.maximum(ri, WINDOW - first)
        hi = jnp.minimum(ri + 2 * WINDOW, nsp * TOK - 1 + WINDOW - first)
        bias[...] = jnp.where((ci >= lo) & (ci <= hi), 0.0, -jnp.inf)
        rows = pl.multiple_of(b * BLK, 32)
        half = lax.broadcasted_iota(jnp.int32, (BLK, 128), 1) < 64

        def tile(t, carry):
            qt = qr[t, pl.ds(rows, BLK), :]
            acc, ends = None, []
            for par in range(2):
                i = (t // 2) * 2 + par
                sc = nt(qt, kk[i, pl.ds(rows, QW), :]) * 0.125 + bias[...]
                snk = sink[2 * t + par]
                top = jnp.maximum(jnp.max(sc, axis=1, keepdims=True), snk)
                prob = jnp.exp(sc - top).astype(BF)
                part = mm(prob, vv[i, pl.ds(rows, QW), :])
                acc = part if acc is None else acc + part
                ends.append(jnp.exp(snk - top))
            den = acc[:, 128:] + jnp.where(half, ends[0], ends[1])
            att[:, pl.ds(pl.multiple_of(t * 128, 128), 128)] = (acc[:, :128] / den).astype(BF)
            return carry

        lax.fori_loop(0, 4, tile, 0, unroll=True)

    UP, LOW = 0, 1
    at_half = {("n", LOW): 0, ("p", UP): 1, ("f", UP): 2, ("f", LOW): 3, ("n", UP): 4, ("p", LOW): 5, ("o", UP): 6, ("o", LOW): 7}
    ahead = {1: "n", -1: "p"}
    back = {1: "p", -1: "n"}
    via = {1: UP, -1: LOW}
    cols_in = {tag: [pl.ds(i * (D // n), D // n) for i in range(n)] for tag, n in SUB.items()}
    cols_of = cols_in["r1"]

    def project(block):
        def cols(n, carry):
            at_n = pl.ds(pl.multiple_of(n * 512, 512), 512)
            done = mm(att[...], ow[:, at_n]).astype(BF)
            for part in (UP, LOW):
                pb1[at_half[block, part], :, at_n] = done[part * HALF : (part + 1) * HALF]
            return carry

        lax.fori_loop(0, 4, cols, 0)

    def rs_far(tag, pb, sbuf):
        for i, cols in enumerate(cols_in[tag]):
            for r in (1, -1):
                key = (tag, "s", i) if tag == "r2" else (tag, "s", r, i)
                send(key, tag, pb.at[at_half["f", via[r]], :, cols], ydev[r], sbuf.at[via[r], :, cols])

    def sum_key(tag, part, i):
        return (tag, "f", i if tag == "r2" else part)

    def rs_near(tag, pb, fbuf, r, i):
        part, cols = 1 - via[r], cols_in[tag][i]
        send(sum_key(tag, part, i), tag, pb.at[at_half[ahead[r], part], :, cols], ydev[r], fbuf.at[part, via[r], :, cols])

    def rs_relay(tag, pb, sbuf, fbuf, r, i):
        cols, part = cols_in[tag][i], via[r]
        j = at_half[ahead[r], part]
        if tag == "r1":
            recv((tag, "s", r, i), sbuf.at[part, :, cols])
        pb[j, :, cols] = (pb[j, :, cols].astype(F32) + sbuf[part, :, cols].astype(F32)).astype(BF)
        send(sum_key(tag, part, i), tag, pb.at[j, :, cols], ydev[r], fbuf.at[part, via[r], :, cols])

    def rs_sum(pb, fbuf, part, cols):
        own = pb[at_half["o", part], :, cols].astype(F32)
        return own + fbuf[part, 0, :, cols].astype(F32) + fbuf[part, 1, :, cols].astype(F32)

    ynext = {"f": (y + 2) % NY, "n": (y + 1) % NY, "p": (y + NY - 1) % NY, "o": y}

    def normalise(part):
        rows = pl.ds(part * HALF, HALF)
        recv(sum_key("r1", part, 0), pb1.at[pl.ds(0, 2)])
        total = st[rows, :].astype(F32) + rs_sum(pb1, f1, part, slice(None))
        mixed[rows, :] = total.astype(BF)
        wide = mixed[rows, :].astype(F32)
        scale = lax.rsqrt(jnp.mean(wide * wide, axis=1, keepdims=True) + 1e-06)
        xs[at_half["o", part]] = (wide * scale * gain[...]).astype(BF)

    def g_cols(part):
        return cols_of if part == LOW else [pl.ds(0, D)]

    def g_send(part):
        for i, cols in enumerate(g_cols(part)):
            for r in (1, -1):
                send(("g", part, i), "g", xs.at[at_half["o", part], :, cols], ydev[r], xs.at[at_half[back[r], part], :, cols])

    def g_recv(part, i):
        cols = g_cols(part)[i]
        recv(("g", part, i), xs.at[pl.ds(0, 2), :, cols])
        for r in (1, -1):
            if via[r] == part:
                ref = xs.at[at_half[back[r], part], :, cols]
                send(("gh",), "g", ref, ydev[r], xs.at[at_half["f", part], :, cols])

    def g_far():
        recv(("gh",), xs.at[pl.ds(0, 2)])

    def gate_up(first, count):
        many = count * HALF
        rows = pl.ds(0, many)

        def act(gate, upward):
            return (gate / (1.0 + jnp.exp(-gate)) * upward).astype(BF)

        def cols(n, carry):
            gu = []
            for base in (0, GB):
                w = wb[:, :, :, :, pl.ds(pl.multiple_of(base + n * 256, 256), 256)].reshape(D, 256)
                gu.append(mm(xs[first : first + count].reshape(many, D), w))
            hid[rows, pl.ds(pl.multiple_of(n * 256, 256), 256)] = act(*gu)
            return carry

        gu = mm(xs[first : first + count].reshape(many, D), wa[:, :, :, :, : 2 * rest].reshape(D, 2 * rest))
        hid[rows, GB:] = act(gu[:, :rest], gu[:, rest:])
        lax.fori_loop(0, GB // 256, cols, 0, unroll=True)

    def over(n, dz):
        zz = (z + dz + NZ) % NZ
        act = xs[0:2, :, pl.ds(pl.multiple_of(zz * 256, 256), 256)].reshape(BLK, 256)
        if n < CB // 256:
            w = wb[zz, :, :, :, 256 * n : 256 * (n + 1)]
        else:
            w = wa[zz, :, :, :, : 2 * rest]
        return mm(act, w.reshape(256, 256))

    def early():
        mates(2)
        for n in range(CB // 256 + 1):
            acc = over(n, 0)
            for dz in (1, -1, 2, -2):
                acc = acc + over(n, dz)
            pre[n] = acc

    def early_more():
        mates(3)
        for n in range(CB // 256 + 1):
            pre[n] = pre[n] + over(n, 3) + over(n, -3)

    def late():
        mates(4)
        parts_of = GB // 256

        def total(n):
            return pre[n] + over(n, 4)

        def act(gate, upward):
            return (gate / (1.0 + jnp.exp(-gate)) * upward).astype(BF)

        for n in range(parts_of):
            hid[:BLK, 256 * n : 256 * (n + 1)] = act(total(n), total(parts_of + n))
        gu = total(2 * parts_of)
        hid[:BLK, GB:] = act(gu[:, :rest], gu[:, rest:])

    def down(first, count, i):
        many = count * HALF

        def cols(n, carry):
            at_n = pl.ds(pl.multiple_of(i * (D // SUB["r2"]) + n * 512, 512), 512)
            done = mm(hid[pl.ds(0, many), :], dt[:, at_n]).astype(BF)
            pb2[first : first + count, :, at_n] = done.reshape(count, HALF, 512)
            return carry

        lax.fori_loop(0, D // SUB["r2"] // 512, cols, 0, unroll=True)

    def near2(i):
        down(0, 2, i)
        for r in (1, -1):
            rs_near("r2", pb2, f2, r, i)

    def far2():
        g_far()
        gate_up(2, 2)
        for i in range(SUB["r2"]):
            down(2, 2, i)
        rs_far("r2", pb2, s2)

    def own2():
        gate_up(4, 4)
        for i in range(SUB["r2"]):
            down(4, 4, i)

    def near1(r):
        for i in range(SUB["r1"]):
            rs_near("r1", pb1, f1, r, i)

    def relay2(i):
        recv(("r2", "s", i), s2.at[:, :, cols_in["r2"][i]])
        for r in (1, -1):
            rs_relay("r2", pb2, s2, f2, r, i)

    def attend_on(block):
        if block == "f":
            loaded("sink", sink)
        if block == "o":
            loaded("st", st)
            loaded("gain", gain)
        attend(ynext[block])

    def project_on(block):
        if block == "f":
            loaded("ow", ow)
        project(block)
        if block == "f":
            rs_far("r1", pb1, s1)
        if block == "p":
            near1(-1)

    def norm_on(part):
        normalise(part)
        g_send(part)

    steps = {
        "begin": begin,
        "turn_q": turn_q,
        "prep_own": prepare_own,
        "prepare": prepare_ends,
        "near+": lambda: near1(1),
        "norm_U": lambda: norm_on(UP),
        "norm_L": lambda: norm_on(LOW),
        "gU": lambda: g_recv(UP, 0),
        "gL0": lambda: g_recv(LOW, 0),
        "gL1": lambda: g_recv(LOW, 1),
        "ax_mid": ax_mid,
        "ax_end": ax_end,
        "early1": early,
        "feed1": late,
        "early2": early_more,
        "feed2": far2,
        "feed3": own2,
    }

    def run_steps(name):
        if name in steps:
            return steps[name]()
        if name[:-1] in ("near", "r2l", "fin"):
            return {"near": near2, "r2l": relay2, "fin": finish}[name[:-1]](int(name[-1]))
        head, *rest_of = name.split("_")
        if head == "att":
            return attend_on(rest_of[0])
        if head == "proj":
            return project_on(rest_of[0])
        if head[:2] == "rl":
            return rs_relay("r1", pb1, s1, f1, 1 if head[2] == "+" else -1, int(head[3]))
        numbers = [int(n) for n in rest_of]
        return {"bz": bz, "bm": bx_mid, "be": bx_end, "az": az, "tr": turn_down}[head](*numbers)

    def finish(i):
        cols = cols_in["r2"][i]
        recv(("r2", "f", i), pb2.at[pl.ds(0, 4), :, cols])
        for part in (UP, LOW):
            rows = pl.ds(part * HALF, HALF)
            res[rows, cols] = (mixed[rows, cols].astype(F32) + 0.5 * rs_sum(pb2, f2, part, cols)).astype(BF)
        pltpu.make_async_copy(res.at[:, cols], out.at[:, cols], osem).start()

    for name in ORDER:
        run_steps(name)

    def drain():
        everything = {
            "halo": kv.at[:, pl.ds(0, 2 * WINDOW)],
            "bz": wb.at[pl.ds(0, 6), 0, 0], "bzh": oneb, "bx": wb.at[:, pl.ds(0, 2), 0], "bh": wb.at[:, 0, 0],
            "bm": wb.at[:, :, 0], "ax": twoa, "ah": onea, "az": wa.at[pl.ds(0, 6), :, 0], "azh": wa.at[0, :, 0],
            "am": wa.at[:, :, 0], "r1": pb1.at[pl.ds(0, 6)], "r2": pb2.at[pl.ds(0, 6)], "g": xs.at[pl.ds(0, 6)],
        }
        for kind, ref in everything.items():
            pltpu.make_async_copy(ref, ref, ssem.at[given[kind]]).wait()

    drain()
    pltpu.make_async_copy(res, out, osem).wait()
    assert len(taken) == NRECV and len(given) == NSEND, (len(taken), len(given))


def local(queries, keys, values, sink, stream, out_weight, norm_gain, gate_weight, up_weight, down_weight):
    hbm = pl.BlockSpec(memory_space=pltpu.HBM)
    V = pltpu.VMEM
    done = pl.pallas_call(
        kernel,
        name="layer",
        out_shape=jax.ShapeDtypeStruct((BLK, D), BF),
        in_specs=[hbm] * 11,
        out_specs=hbm,
        scratch_shapes=[
            V((NZ, NX, NC, ROWS, CA), BF),
            V((NZ, NX, NC, ROWS, CB), BF),
            V((2 * EXT + 2 * NZ * NX * NC, 128), F32),
            V((TOK, 512), BF),
            V((4, TOK, 128), BF),
            V((2, EXT, 128), BF),
            V((4, PAD, 128), BF),
            V((4, PAD, 256), BF),
            V((512, D), BF),
            V((BLK, D), BF),
            V((BLK, QW), F32),
            V((BLK, 512), BF),
            V((8, HALF, D), BF),
            V((2, HALF, D), BF),
            V((2, 2, HALF, D), BF),
            V((8, HALF, D), BF),
            V((2, HALF, D), BF),
            V((2, 2, HALF, D), BF),
            V((BLK, D), BF),
            V((8, HALF, D), BF),
            V((2 * BLK, FFL), BF),
            V((FFL, D), BF),
            V((CB // 256 + 1, BLK, 256), F32),
            V((1, D), F32),
            pltpu.SMEM((8,), F32),
            V((BLK, D), BF),
            pltpu.SemaphoreType.DMA((9,)),
            pltpu.SemaphoreType.DMA((NSEND,)),
            pltpu.SemaphoreType.DMA((NRECV,)),
            pltpu.SemaphoreType.DMA,
        ],
        compiler_params=pltpu.CompilerParams(
            collective_id=0, has_side_effects=True, vmem_limit_bytes=62 * 1024 * 1024
        ),
    )(
        queries, keys, values, sink, stream, out_weight, norm_gain.reshape(1, D),
        gate_weight, up_weight, down_weight.T, jnp.asarray(tables()),
    )
    return done


def solution(mesh):
    placed = (
        P("sp", "tp"), P("sp", "tp"), P("sp", "tp"), P("tp"), P(("sp", "tp"), None), P("tp", None), P(),
        P("sp", "tp"), P("sp", "tp"), P("tp", "sp"),
    )
    return jax.shard_map(local, mesh=mesh, in_specs=placed, out_specs=P(("sp", "tp"), None), check_vma=False)
```

```python
import jax
import jax.numpy as jnp
import numpy as np
from jax import lax
from jax.experimental import pallas as pl
from jax.experimental.pallas import tpu as pltpu
from jax.sharding import PartitionSpec as P

HEAD = 64
WINDOW = 128
MESH = pl.DeviceIdType.MESH
BF = jnp.bfloat16
F32 = jnp.float32

NZ, NX, NC, NY = 8, 4, 2, 4
ROWS = 32
TOK = 640
BLK = TOK // NY
HALF = BLK // 2
EXT = TOK + 2 * WINDOW
PAD = 3 * BLK + 4 * WINDOW
D = 2048
FFL = 1408
GB = 1280
CB = 2 * GB
CA = 2 * (FFL - GB) + FFL
QW = 512
NRECV = 68
NSEND = 8
ORDER = (
    "begin", "turn_q", "prep_own", "prepare", "att_f", "proj_f", "bz_1", "att_n", "proj_n", "att_p", "az_1_0",
    "ax_mid", "proj_p", "att_o", "proj_o", "rl+0", "bm_1", "bz_2", "rl-0", "bm_0", "az_2_0", "rl+1", "near+", "rl-1",
    "bm_-1", "ax_end", "az_1_1", "tr_0", "be_1", "az_1_-1", "bm_2", "bz_3", "norm_U", "az_3_0", "bm_-2", "az_1_2",
    "be_0", "tr_1", "tr_-1", "be_-1", "az_2_1", "norm_L", "be_2", "az_2_-1", "bz_4", "bm_3", "az_4_0", "gU",
    "az_2_2", "bm_-3", "tr_2", "tr_-2", "az_3_1", "be_-2", "gL0", "az_3_-1", "bm_4", "az_3_2", "gL1", "early1",
    "tr_3", "be_3", "az_4_1", "tr_-3", "az_4_-1", "be_-3", "az_4_2", "early2", "be_4", "tr_4", "feed1", "near0",
    "near1", "near2", "near3", "feed2", "feed3", "r2l0", "r2l1", "r2l2", "r2l3", "fin0", "fin1", "fin2", "fin3",
)
SUB = {"r1": 2, "r2": 4}


def tables():
    lane = (np.arange(128) % 64) % 32
    freq = 1.0 / 10000.0 ** (2.0 * lane / HEAD)
    near = (np.arange(EXT) - WINDOW)[:, None] * freq[None]
    far = (np.arange(NZ * NX * NC) * TOK)[:, None] * freq[None]
    return np.concatenate([np.cos(near), np.sin(near), np.cos(far), np.sin(far)], 0).astype(np.float32)


def nt(a, b):
    return lax.dot_general(a, b, (((1,), (1,)), ((), ())), preferred_element_type=F32)


def mm(a, b):
    return jnp.dot(a, b, preferred_element_type=F32)


def kernel(
    q_hbm, k_hbm, v_hbm, sink_hbm, st_hbm, ow_hbm, gain_hbm, g_hbm, u_hbm, d_hbm, tab_hbm,
    out,
    wa, wb, tab, q, qr, kv, kk, vv, ow, st, bias, att,
    pb1, s1, f1, pb2, s2, f2, mixed, xs, hid, dt, pre, gain, sink, res,
    lsem, ssem, rsem, osem,
):
    s = lax.axis_index("sp")
    y = lax.axis_index("tp")
    c = s % NC
    x = (s // NC) % NX
    z = s // (NC * NX)

    def at(zz, xx, cc):
        return ((zz % NZ) * NX + xx % NX) * NC + cc

    ydev = {1: (s, (y + 1) % NY), -1: (s, (y + NY - 1) % NY)}
    xdev = {1: (at(z, x + 1, c), y), -1: (at(z, x + NX - 1, c), y)}
    zdev = {1: (at(z + 1, x, c), y), -1: (at(z + NZ - 1, x, c), y)}
    mate = (at(z, x, 1 - c), y)
    nsp = NZ * NX * NC
    hdev = {1: ((s + 1) % nsp, y), -1: ((s + nsp - 1) % nsp, y)}

    barrier = pltpu.get_barrier_semaphore()
    for dev in (*ydev.values(), *xdev.values(), *zdev.values(), mate, *hdev.values()):
        pl.semaphore_signal(barrier, inc=1, device_id=dev, device_id_type=MESH)

    loads = {}

    def load(name, src, dst):
        i = loads.setdefault(name, len(loads))
        pltpu.make_async_copy(src, dst, lsem.at[i]).start()

    def loaded(name, ref):
        pltpu.make_async_copy(ref, ref, lsem.at[loads[name]]).wait()

    rest = FFL - GB
    load("kv", k_hbm, kv.at[0, pl.ds(WINDOW, TOK)])
    load("kv", v_hbm, kv.at[1, pl.ds(WINDOW, TOK)])
    load("b", g_hbm.at[:, pl.ds(0, GB)], wb.at[z, x, c, :, pl.ds(0, GB)])
    load("b", u_hbm.at[:, pl.ds(0, GB)], wb.at[z, x, c, :, pl.ds(GB, GB)])
    load("a", d_hbm, wa.at[z, x, c, :, pl.ds(2 * rest, FFL)])
    load("a", g_hbm.at[:, pl.ds(GB, rest)], wa.at[z, x, c, :, pl.ds(0, rest)])
    load("a", u_hbm.at[:, pl.ds(GB, rest)], wa.at[z, x, c, :, pl.ds(rest, rest)])
    load("tab", tab_hbm, tab)
    load("q", q_hbm, q)
    load("ow", ow_hbm, ow)
    load("st", st_hbm, st)
    load("gain", gain_hbm, gain)
    load("sink", sink_hbm, sink)

    def greet():
        pl.semaphore_wait(barrier, 9)

    greet()

    taken, given = {}, {}

    def send(key, kind, ref, dev, dst=None):
        i = taken.setdefault(key, len(taken))
        k = given.setdefault(kind, len(given))
        pltpu.make_async_remote_copy(
            src_ref=ref, dst_ref=ref if dst is None else dst, send_sem=ssem.at[k], recv_sem=rsem.at[i],
            device_id=dev, device_id_type=MESH,
        ).start()

    def recv(key, ref):
        i = taken.setdefault(key, len(taken))
        pltpu.make_async_copy(ref, ref, rsem.at[i]).wait()

    def zb(dz, half=None):
        ref = wb.at[(z + dz + NZ) % NZ, x, c]
        return ref if half is None else ref.at[pl.ds(16 * half, 16)]

    def xb(dz, dx, half=None):
        ref = wb.at[(z + dz + NZ) % NZ, (x + dx + NX) % NX, c]
        return ref if half is None else ref.at[pl.ds(16 * half, 16)]

    def za(dz, dx, half=None):
        ref = wa.at[(z + dz + NZ) % NZ, (x + dx + NX) % NX, c]
        return ref if half is None else ref.at[pl.ds(16 * half, 16)]

    def xa(dx, half=None):
        ref = wa.at[z, (x + dx + NX) % NX, c]
        return ref if half is None else ref.at[pl.ds(16 * half, 16)]

    oneb, onea = wb.at[0, 0, 0], wa.at[0, 0, 0]
    twob, twoa = wb.at[pl.ds(0, 2), 0, 0], wa.at[pl.ds(0, 2), 0, 0]
    way = ((1, 0), (-1, 1))

    def b_mate(dz, dx):
        send(("bm", max(abs(dz), 2)), "bx", xb(dz, dx), mate)

    def a_mate(dz, dx):
        send(("am", dz), "az", za(dz, dx), mate)

    def bx_send(dz):
        for r in (1, -1):
            send(("bx", dz), "bx", xb(dz, 0), xdev[r])
        b_mate(dz, 0)

    def bx_mid(dz):
        recv(("bx", dz), twob)
        for r, half in way:
            send(("bh", dz), "bz", xb(dz, -r, half), xdev[r])
        for r in (1, -1):
            b_mate(dz, r)

    def bx_end(dz):
        recv(("bh", dz), oneb)
        b_mate(dz, 2)

    def bz(n):
        recv(("bz", n), twob if n < 4 else oneb)
        for r, half in way:
            if n < 3:
                send(("bz", n + 1), "bz", zb(-r * n), zdev[r])
            elif n == 3:
                send(("bz", 4), "bz", zb(-r * 3, half), zdev[r])
        for dz in (n, -n) if n < 4 else (4,):
            bx_send(dz)

    def az_send(n, dx, r):
        if n < 4:
            send(("az", n, dx), "az", za(-r * (n - 1), dx), zdev[r])
        else:
            send(("az", 4, dx), "ax", za(-r * 3, dx, 0 if r == 1 else 1), zdev[r])

    def az(n, dx):
        recv(("az", n, dx), twoa if n < 4 else onea)
        for r in (1, -1):
            if n < 4:
                az_send(n + 1, dx, r)
        for dz in (n, -n) if n < 4 else (4,):
            a_mate(dz, dx)

    def ax_mid():
        recv(("ax",), twoa)
        for r, half in way:
            send(("ah",), "ax", xa(-r, half), xdev[r])
        for r in (1, -1):
            for dx in (1, -1):
                az_send(1, dx, r)
        for r in (1, -1):
            a_mate(0, r)

    def ax_end():
        recv(("ah",), onea)
        for r in (1, -1):
            az_send(1, 2, r)
        a_mate(0, 2)

    def turn_down(dz):
        zz = (z + dz + NZ) % NZ
        recv(("am", dz), wa.at[0, :, 0])
        dt[:, pl.ds(pl.multiple_of(zz * 256, 256), 256)] = wa[zz, :, :, :, 2 * rest :].reshape(256, FFL).T

    def mates(n):
        recv(("bm", n), wb.at[pl.ds(0, {2: 5, 3: 2, 4: 1}[n]), :, 0])

    def begin():
        loaded("kv", kv.at[:, pl.ds(0, TOK)])
        send(("halo",), "halo", kv.at[:, pl.ds(WINDOW, WINDOW)], hdev[-1], kv.at[:, pl.ds(WINDOW + TOK, WINDOW)])
        send(("halo",), "halo", kv.at[:, pl.ds(TOK, WINDOW)], hdev[1], kv.at[:, pl.ds(0, WINDOW)])
        loaded("b", oneb)
        loaded("a", onea)
        for r in (1, -1):
            send(("bz", 1), "bz", zb(0), zdev[r])
            send(("ax",), "ax", xa(0), xdev[r])
        for r in (1, -1):
            az_send(1, 0, r)
        bx_send(0)
        a_mate(0, 0)

    loaded("tab", tab)
    cb = tab[pl.ds(2 * EXT + s, 1), :]
    sb = tab[pl.ds(2 * EXT + nsp + s, 1), :]

    def rotate(rows, value):
        cl, sl = tab[rows, :], tab[pl.ds(EXT + rows.start, rows.size), :]
        cos = cb * cl - sb * sl
        sin = sb * cl + cb * sl
        return value.astype(F32) * cos + mm(value, turn) * sin

    jj = lax.broadcasted_iota(jnp.int32, (128, 128), 0)
    ii = lax.broadcasted_iota(jnp.int32, (128, 128), 1)
    low = (ii % 64) < 32
    turn = (jnp.where(jj == ii - 32, jnp.where(low, 0.0, 1.0), 0.0)
            - jnp.where(jj == ii + 32, jnp.where(low, 1.0, 0.0), 0.0)).astype(BF)
    flip = jnp.where((jj + 64) % 128 == ii, 1.0, 0.0).astype(BF)

    def turn_q():
        loaded("q", q)
        for t in range(4):
            qr[t] = rotate(pl.ds(WINDOW, TOK), q[:, 128 * t : 128 * (t + 1)]).astype(BF)

    def prepare(first, many):
        rows = pl.ds(first, many)
        lane = lax.broadcasted_iota(jnp.int32, (many, 128), 1)
        left = lane < 64
        kr = rotate(rows, kv[0, rows]).astype(BF)
        ks = mm(kr, flip)
        kr = kr.astype(F32)
        vr = kv[1, rows].astype(F32)
        vs = mm(kv[1, rows], flip)
        for i in range(4):
            ksrc, vsrc = ((kr, vr), (ks, vs), (ks, vs), (kr, vr))[i]
            keep = left if i % 2 == 0 else lane >= 64
            kk[i, rows, :] = jnp.where(keep, ksrc, 0.0).astype(BF)
            vv[i, rows, :128] = jnp.where(keep, vsrc, 0.0).astype(BF)

    def prepare_own():
        left = lax.broadcasted_iota(jnp.int32, (EXT, 128), 1) < 64
        one = jnp.where(left, 1.0, 0.0).astype(BF)
        two = jnp.where(left, 0.0, 1.0).astype(BF)
        for i in range(4):
            kk[i, EXT:, :] = jnp.zeros((PAD - EXT, 128), BF)
            vv[i, EXT:, :] = jnp.zeros((PAD - EXT, 256), BF)
            vv[i, :EXT, 128:] = one if i % 2 == 0 else two
        prepare(WINDOW, TOK)

    def prepare_ends():
        recv(("halo",), kv.at[:, pl.ds(0, 2 * WINDOW)])
        prepare(0, WINDOW)
        prepare(WINDOW + TOK, WINDOW)

    def attend(b):
        first = s * TOK + b * BLK
        ri = lax.broadcasted_iota(jnp.int32, (BLK, QW), 0)
        ci = lax.broadcasted_iota(jnp.int32, (BLK, QW), 1)
        lo = jnp.maximum(ri, WINDOW - first)
        hi = jnp.minimum(ri + 2 * WINDOW, nsp * TOK - 1 + WINDOW - first)
        bias[...] = jnp.where((ci >= lo) & (ci <= hi), 0.0, -jnp.inf)
        rows = pl.multiple_of(b * BLK, 32)
        half = lax.broadcasted_iota(jnp.int32, (BLK, 128), 1) < 64

        def tile(t, carry):
            qt = qr[t, pl.ds(rows, BLK), :]
            acc, ends = None, []
            for par in range(2):
                i = (t // 2) * 2 + par
                sc = nt(qt, kk[i, pl.ds(rows, QW), :]) * 0.125 + bias[...]
                snk = sink[2 * t + par]
                top = jnp.maximum(jnp.max(sc, axis=1, keepdims=True), snk)
                prob = jnp.exp(sc - top).astype(BF)
                part = mm(prob, vv[i, pl.ds(rows, QW), :])
                acc = part if acc is None else acc + part
                ends.append(jnp.exp(snk - top))
            den = acc[:, 128:] + jnp.where(half, ends[0], ends[1])
            att[:, pl.ds(pl.multiple_of(t * 128, 128), 128)] = (acc[:, :128] / den).astype(BF)
            return carry

        lax.fori_loop(0, 4, tile, 0, unroll=True)

    UP, LOW = 0, 1
    at_half = {("n", LOW): 0, ("p", UP): 1, ("f", UP): 2, ("f", LOW): 3, ("n", UP): 4, ("p", LOW): 5, ("o", UP): 6, ("o", LOW): 7}
    ahead = {1: "n", -1: "p"}
    back = {1: "p", -1: "n"}
    via = {1: UP, -1: LOW}
    cols_in = {tag: [pl.ds(i * (D // n), D // n) for i in range(n)] for tag, n in SUB.items()}
    cols_of = cols_in["r1"]

    def project(block):
        def cols(n, carry):
            at_n = pl.ds(pl.multiple_of(n * 512, 512), 512)
            done = mm(att[...], ow[:, at_n]).astype(BF)
            for part in (UP, LOW):
                pb1[at_half[block, part], :, at_n] = done[part * HALF : (part + 1) * HALF]
            return carry

        lax.fori_loop(0, 4, cols, 0, unroll=True)

    def rs_far(tag, pb, sbuf):
        for i, cols in enumerate(cols_in[tag]):
            for r in (1, -1):
                key = (tag, "s", i) if tag == "r2" else (tag, "s", r, i)
                send(key, tag, pb.at[at_half["f", via[r]], :, cols], ydev[r], sbuf.at[via[r], :, cols])

    def sum_key(tag, part, i):
        return (tag, "f", i if tag == "r2" else part)

    def rs_near(tag, pb, fbuf, r, i):
        part, cols = 1 - via[r], cols_in[tag][i]
        send(sum_key(tag, part, i), tag, pb.at[at_half[ahead[r], part], :, cols], ydev[r], fbuf.at[part, via[r], :, cols])

    def rs_relay(tag, pb, sbuf, fbuf, r, i):
        cols, part = cols_in[tag][i], via[r]
        j = at_half[ahead[r], part]
        if tag == "r1":
            recv((tag, "s", r, i), sbuf.at[part, :, cols])
        pb[j, :, cols] = (pb[j, :, cols].astype(F32) + sbuf[part, :, cols].astype(F32)).astype(BF)
        send(sum_key(tag, part, i), tag, pb.at[j, :, cols], ydev[r], fbuf.at[part, via[r], :, cols])

    def rs_sum(pb, fbuf, part, cols):
        own = pb[at_half["o", part], :, cols].astype(F32)
        return own + fbuf[part, 0, :, cols].astype(F32) + fbuf[part, 1, :, cols].astype(F32)

    ynext = {"f": (y + 2) % NY, "n": (y + 1) % NY, "p": (y + NY - 1) % NY, "o": y}

    def normalise(part):
        rows = pl.ds(part * HALF, HALF)
        recv(sum_key("r1", part, 0), pb1.at[pl.ds(0, 2)])
        total = st[rows, :].astype(F32) + rs_sum(pb1, f1, part, slice(None))
        mixed[rows, :] = total.astype(BF)
        wide = mixed[rows, :].astype(F32)
        scale = lax.rsqrt(jnp.mean(wide * wide, axis=1, keepdims=True) + 1e-06)
        xs[at_half["o", part]] = (wide * scale * gain[...]).astype(BF)

    def g_cols(part):
        return cols_of if part == LOW else [pl.ds(0, D)]

    def g_send(part):
        for i, cols in enumerate(g_cols(part)):
            for r in (1, -1):
                send(("g", part, i), "g", xs.at[at_half["o", part], :, cols], ydev[r], xs.at[at_half[back[r], part], :, cols])

    def g_recv(part, i):
        cols = g_cols(part)[i]
        recv(("g", part, i), xs.at[pl.ds(0, 2), :, cols])
        for r in (1, -1):
            if via[r] == part:
                ref = xs.at[at_half[back[r], part], :, cols]
                send(("gh",), "g", ref, ydev[r], xs.at[at_half["f", part], :, cols])

    def g_far():
        recv(("gh",), xs.at[pl.ds(0, 2)])

    def gate_up(first, count):
        many = count * HALF
        rows = pl.ds(0, many)

        def act(gate, upward):
            return (gate / (1.0 + jnp.exp(-gate)) * upward).astype(BF)

        def cols(n, carry):
            gu = []
            for base in (0, GB):
                w = wb[:, :, :, :, pl.ds(pl.multiple_of(base + n * 256, 256), 256)].reshape(D, 256)
                gu.append(mm(xs[first : first + count].reshape(many, D), w))
            hid[rows, pl.ds(pl.multiple_of(n * 256, 256), 256)] = act(*gu)
            return carry

        gu = mm(xs[first : first + count].reshape(many, D), wa[:, :, :, :, : 2 * rest].reshape(D, 2 * rest))
        hid[rows, GB:] = act(gu[:, :rest], gu[:, rest:])
        lax.fori_loop(0, GB // 256, cols, 0, unroll=True)

    def over(n, dz):
        zz = (z + dz + NZ) % NZ
        act = xs[0:2, :, pl.ds(pl.multiple_of(zz * 256, 256), 256)].reshape(BLK, 256)
        if n < CB // 256:
            w = wb[zz, :, :, :, 256 * n : 256 * (n + 1)]
        else:
            w = wa[zz, :, :, :, : 2 * rest]
        return mm(act, w.reshape(256, 256))

    def early():
        mates(2)
        for n in range(CB // 256 + 1):
            acc = over(n, 0)
            for dz in (1, -1, 2, -2):
                acc = acc + over(n, dz)
            pre[n] = acc

    def early_more():
        mates(3)
        for n in range(CB // 256 + 1):
            pre[n] = pre[n] + over(n, 3) + over(n, -3)

    def late():
        mates(4)
        parts_of = GB // 256

        def total(n):
            return pre[n] + over(n, 4)

        def act(gate, upward):
            return (gate / (1.0 + jnp.exp(-gate)) * upward).astype(BF)

        for n in range(parts_of):
            hid[:BLK, 256 * n : 256 * (n + 1)] = act(total(n), total(parts_of + n))
        gu = total(2 * parts_of)
        hid[:BLK, GB:] = act(gu[:, :rest], gu[:, rest:])

    def down(first, count, i):
        many = count * HALF

        def cols(n, carry):
            at_n = pl.ds(pl.multiple_of(i * (D // SUB["r2"]) + n * 512, 512), 512)
            done = mm(hid[pl.ds(0, many), :], dt[:, at_n]).astype(BF)
            pb2[first : first + count, :, at_n] = done.reshape(count, HALF, 512)
            return carry

        lax.fori_loop(0, D // SUB["r2"] // 512, cols, 0, unroll=True)

    def near2(i):
        down(0, 2, i)
        for r in (1, -1):
            rs_near("r2", pb2, f2, r, i)

    def far2():
        g_far()
        gate_up(2, 2)
        for i in range(SUB["r2"]):
            down(2, 2, i)
        rs_far("r2", pb2, s2)

    def own2():
        gate_up(4, 4)
        for i in range(SUB["r2"]):
            down(4, 4, i)

    def near1(r):
        for i in range(SUB["r1"]):
            rs_near("r1", pb1, f1, r, i)

    def relay2(i):
        recv(("r2", "s", i), s2.at[:, :, cols_in["r2"][i]])
        for r in (1, -1):
            rs_relay("r2", pb2, s2, f2, r, i)

    def attend_on(block):
        if block == "f":
            loaded("sink", sink)
        if block == "o":
            loaded("st", st)
            loaded("gain", gain)
        attend(ynext[block])

    def project_on(block):
        if block == "f":
            loaded("ow", ow)
        project(block)
        if block == "f":
            rs_far("r1", pb1, s1)
        if block == "p":
            near1(-1)

    def norm_on(part):
        normalise(part)
        g_send(part)

    steps = {
        "begin": begin,
        "turn_q": turn_q,
        "prep_own": prepare_own,
        "prepare": prepare_ends,
        "near+": lambda: near1(1),
        "norm_U": lambda: norm_on(UP),
        "norm_L": lambda: norm_on(LOW),
        "gU": lambda: g_recv(UP, 0),
        "gL0": lambda: g_recv(LOW, 0),
        "gL1": lambda: g_recv(LOW, 1),
        "ax_mid": ax_mid,
        "ax_end": ax_end,
        "early1": early,
        "feed1": late,
        "early2": early_more,
        "feed2": far2,
        "feed3": own2,
    }

    def run_steps(name):
        if name in steps:
            return steps[name]()
        if name[:-1] in ("near", "r2l", "fin"):
            return {"near": near2, "r2l": relay2, "fin": finish}[name[:-1]](int(name[-1]))
        head, *rest_of = name.split("_")
        if head == "att":
            return attend_on(rest_of[0])
        if head == "proj":
            return project_on(rest_of[0])
        if head[:2] == "rl":
            return rs_relay("r1", pb1, s1, f1, 1 if head[2] == "+" else -1, int(head[3]))
        numbers = [int(n) for n in rest_of]
        return {"bz": bz, "bm": bx_mid, "be": bx_end, "az": az, "tr": turn_down}[head](*numbers)

    def finish(i):
        cols = cols_in["r2"][i]
        recv(("r2", "f", i), pb2.at[pl.ds(0, 4), :, cols])
        for part in (UP, LOW):
            rows = pl.ds(part * HALF, HALF)
            res[rows, cols] = (mixed[rows, cols].astype(F32) + 0.5 * rs_sum(pb2, f2, part, cols)).astype(BF)
        pltpu.make_async_copy(res.at[:, cols], out.at[:, cols], osem).start()

    for name in ORDER:
        run_steps(name)

    def drain():
        everything = {
            "halo": kv.at[:, pl.ds(0, 2 * WINDOW)],
            "bz": wb.at[pl.ds(0, 5), pl.ds(0, 3), 0], "bx": wb.at[pl.ds(0, 6)],
            "ax": wa.at[pl.ds(0, 7), 0, 0], "az": wa.at[pl.ds(0, 7)],
            "r1": pb1.at[pl.ds(0, 6)], "r2": pb2.at[pl.ds(0, 6)], "g": xs.at[pl.ds(0, 6)],
        }
        for kind, ref in everything.items():
            pltpu.make_async_copy(ref, ref, ssem.at[given[kind]]).wait()

    drain()
    pltpu.make_async_copy(res, out, osem).wait()
    assert len(taken) == NRECV and len(given) == NSEND, (len(taken), len(given))


def local(queries, keys, values, sink, stream, out_weight, norm_gain, gate_weight, up_weight, down_weight):
    hbm = pl.BlockSpec(memory_space=pltpu.HBM)
    V = pltpu.VMEM
    done = pl.pallas_call(
        kernel,
        name="layer",
        out_shape=jax.ShapeDtypeStruct((BLK, D), BF),
        in_specs=[hbm] * 11,
        out_specs=hbm,
        scratch_shapes=[
            V((NZ, NX, NC, ROWS, CA), BF),
            V((NZ, NX, NC, ROWS, CB), BF),
            V((2 * EXT + 2 * NZ * NX * NC, 128), F32),
            V((TOK, 512), BF),
            V((4, TOK, 128), BF),
            V((2, EXT, 128), BF),
            V((4, PAD, 128), BF),
            V((4, PAD, 256), BF),
            V((512, D), BF),
            V((BLK, D), BF),
            V((BLK, QW), F32),
            V((BLK, 512), BF),
            V((8, HALF, D), BF),
            V((2, HALF, D), BF),
            V((2, 2, HALF, D), BF),
            V((8, HALF, D), BF),
            V((2, HALF, D), BF),
            V((2, 2, HALF, D), BF),
            V((BLK, D), BF),
            V((8, HALF, D), BF),
            V((2 * BLK, FFL), BF),
            V((FFL, D), BF),
            V((CB // 256 + 1, BLK, 256), F32),
            V((1, D), F32),
            pltpu.SMEM((8,), F32),
            V((BLK, D), BF),
            pltpu.SemaphoreType.DMA((9,)),
            pltpu.SemaphoreType.DMA((NSEND,)),
            pltpu.SemaphoreType.DMA((NRECV,)),
            pltpu.SemaphoreType.DMA,
        ],
        compiler_params=pltpu.CompilerParams(
            collective_id=0, has_side_effects=True, vmem_limit_bytes=62 * 1024 * 1024
        ),
    )(
        queries, keys, values, sink, stream, out_weight, norm_gain.reshape(1, D),
        gate_weight, up_weight, down_weight.T, jnp.asarray(tables()),
    )
    half = BLK // 2

    def copy_out(src, dst, held, sems):
        for way in range(2):
            for i in range(2):
                rows = pl.ds(i * half, half)
                if way:
                    pltpu.make_async_copy(src.at[rows], held.at[rows], sems.at[0, i]).wait()
                    pltpu.make_async_copy(held.at[rows], dst.at[rows], sems.at[1, i]).start()
                else:
                    pltpu.make_async_copy(src.at[rows], held.at[rows], sems.at[0, i]).start()
        for i in range(2):
            rows = pl.ds(i * half, half)
            pltpu.make_async_copy(held.at[rows], dst.at[rows], sems.at[1, i]).wait()

    return pl.pallas_call(
        copy_out,
        name="copy_out",
        out_shape=jax.ShapeDtypeStruct((BLK, D), BF),
        in_specs=[hbm],
        out_specs=hbm,
        scratch_shapes=[V((BLK, D), BF), pltpu.SemaphoreType.DMA((2, 2))],
    )(done)


def solution(mesh):
    placed = (
        P("sp", "tp"), P("sp", "tp"), P("sp", "tp"), P("tp"), P(("sp", "tp"), None), P("tp", None), P(),
        P("sp", "tp"), P("sp", "tp"), P("tp", "sp"),
    )
    return jax.shard_map(local, mesh=mesh, in_specs=placed, out_specs=P(("sp", "tp"), None), check_vma=False)
```
